32 devices in a mesh: sp: 8 (over z, x), tp: 4 (over y, core).
Axes of the slice: x: 2, y: 2, z: 4, core: 2. Of those that a mesh axis runs over, the one named last changes fastest.
Arguments:
- queries: bfloat16 [4096, 3072], P('sp', 'tp'), may hold values from -6 to 6
- latent: bfloat16 [4096, 1024], P('sp'), may hold values from -6 to 6
- rope_key: bfloat16 [4096, 64], P('sp'), may hold values from -6 to 6
- key_weight: bfloat16 [1024, 2048], P(None, 'tp'), as said below
- value_weight: bfloat16 [1024, 2048], P(None, 'tp'), as said below
- log_sums: float32 [16, 4096], P('tp', 'sp'), as said below
- attn_out: bfloat16 [4096, 2048], P('sp', 'tp'), as said below
- out_grad: bfloat16 [4096, 2048], P('sp', 'tp'), may hold values from -6 to 6
Outputs:
- d_queries: bfloat16 [4096, 3072], P('sp', 'tp')
- d_latent: float32 [4096, 1024], P('sp')
- d_rope: float32 [4096, 64], P('sp')
- d_value_weight: float32 [1024, 2048], P('sp', 'tp')
The draws below stay inside these ranges and needn't reach their ends.
Inputs may be any that keep to these rules, and one draw needn't show every extreme that they name: `key_weight`: independent entries of order one multiplied by 1024^(-1/2). `value_weight`: independent entries of order one multiplied by 1024^(-1/2). log_sums[h, i] is the logarithm of the sum over j <= i of exp(scores[h, i, j]) of the forward pass. attn_out is the forward pass output: head h of row i is the sum over j <= i of exp(scores - log_sums) rounded to bfloat16, times head h of values row j, rounded to bfloat16.
All inputs are finite; a program needn't handle non-finite values.
Results may differ from the reference program's by a relative error of at most 0.018.
Values may be sent and summed in bfloat16 or wider, within the bound.
A program may use at most 192 MiB of HBM per device.

```python
import jax
import jax.numpy as jnp
from jax import lax

HEADS = 16
NOPE = 128
ROPE = 64
VDIM = 128
LATENT = 1024
TOKENS = 4096


def rough_normal(key, shape):
    return jnp.clip(jax.random.normal(key, shape, jnp.float32), -6.0, 6.0)


def base_inputs(key):
    queries = rough_normal(jax.random.fold_in(key, 101), (TOKENS, HEADS * (NOPE + ROPE)))
    latent = rough_normal(jax.random.fold_in(key, 102), (TOKENS, LATENT))
    rope_key = rough_normal(jax.random.fold_in(key, 103), (TOKENS, ROPE))
    key_weight = rough_normal(jax.random.fold_in(key, 104), (LATENT, HEADS * NOPE)) * LATENT ** (-0.5)
    value_weight = rough_normal(jax.random.fold_in(key, 105), (LATENT, HEADS * VDIM)) * LATENT ** (-0.5)
    return (queries.astype(jnp.bfloat16), latent.astype(jnp.bfloat16), rope_key.astype(jnp.bfloat16), key_weight.astype(jnp.bfloat16), value_weight.astype(jnp.bfloat16))


def forward_outputs(key):
    queries, latent, rope_key, key_weight, value_weight = base_inputs(key)
    head_width = NOPE + ROPE
    score_scale = head_width ** (-0.5)
    key_nope = jnp.dot(latent, key_weight, preferred_element_type=jnp.float32).astype(jnp.bfloat16)
    values = jnp.dot(latent, value_weight, preferred_element_type=jnp.float32).astype(jnp.bfloat16)
    query_heads = queries.reshape(TOKENS, HEADS, head_width).transpose(1, 0, 2)
    key_heads = key_nope.reshape(TOKENS, HEADS, NOPE).transpose(1, 0, 2)
    value_heads = values.reshape(TOKENS, HEADS, VDIM).transpose(1, 0, 2)
    positions = jnp.arange(TOKENS, dtype=jnp.int32)
    causal = positions[None, :] <= positions[:, None]

    def one_head(operands):
        query_h, key_h, value_h = operands
        scores = score_scale * (jnp.dot(query_h[:, :NOPE], key_h.T, preferred_element_type=jnp.float32) + jnp.dot(query_h[:, NOPE:], rope_key.T, preferred_element_type=jnp.float32))
        masked = jnp.where(causal, scores, -jnp.inf)
        log_sum = jax.nn.logsumexp(masked, axis=1)
        attn_probs = jnp.exp(masked - log_sum[:, None]).astype(jnp.bfloat16)
        return (log_sum, jnp.dot(attn_probs, value_h, preferred_element_type=jnp.float32).astype(jnp.bfloat16))
    log_sums, out_heads = lax.map(one_head, (query_heads, key_heads, value_heads))
    return (log_sums, out_heads.transpose(1, 0, 2).reshape(TOKENS, HEADS * VDIM))


def draw_queries(key, part):
    return base_inputs(key)[0]


def draw_latent(key, part):
    return base_inputs(key)[1]


def draw_rope_key(key, part):
    return base_inputs(key)[2]


def draw_key_weight(key, part):
    return base_inputs(key)[3]


def draw_value_weight(key, part):
    return base_inputs(key)[4]


def draw_log_sums(key, part):
    return forward_outputs(key)[0]


def draw_attn_out(key, part):
    return forward_outputs(key)[1]


def strengthened(result, key, source, target, shards_of, factor):
    owner, partner = [(jnp.arange(result.shape[dim]) // (result.shape[dim] // shards_of)).reshape([-1 if axis == dim else 1 for axis in range(result.ndim)]) for dim in (source, target)]
    chosen = jax.random.permutation(key, shards_of)[partner]
    strong = (owner == chosen) | (owner == (partner + shards_of // 2) % shards_of)
    return jnp.where(strong, factor * result, result)


def shard_levels(own_key, dims, pieces, low, top_value):
    loudness = 1.0
    for axis_at, blocks in pieces:
        steps = jax.random.uniform(jax.random.fold_in(jax.random.fold_in(own_key, 6), axis_at), (blocks,), jnp.float32, low / len(pieces), top_value / len(pieces))
        loudness = loudness * jnp.repeat(jnp.exp(steps), dims[axis_at] // blocks).reshape((-1,) + (1,) * (len(dims) - 1 - axis_at))
    return loudness


def noise_with(rng, extent, deviation, reach, split, heavy, kind=jnp.bfloat16):
    drawn = deviation * jax.random.normal(rng, extent, jnp.float32)
    if split:
        drawn = drawn * shard_levels(rng, extent, split, -0.22, 0.18)
    return jnp.clip(strengthened(drawn, jax.random.fold_in(rng, 3), *heavy), -reach, reach).astype(kind)


def setup_inputs(seed: int = 0) -> dict:
    keys = jax.random.split(jax.random.key(seed), 9)
    return {
        "queries": draw_queries(jax.random.fold_in(keys[8], 71), 0),
        "latent": draw_latent(jax.random.fold_in(keys[8], 71), 0),
        "rope_key": draw_rope_key(jax.random.fold_in(keys[8], 71), 0),
        "key_weight": draw_key_weight(jax.random.fold_in(keys[8], 71), 0),
        "value_weight": draw_value_weight(jax.random.fold_in(keys[8], 71), 0),
        "log_sums": draw_log_sums(jax.random.fold_in(keys[8], 71), 0),
        "attn_out": draw_attn_out(jax.random.fold_in(keys[8], 71), 0),
        "out_grad": noise_with(keys[7], (TOKENS, HEADS * VDIM), 1.0, 6.0, ((0, 8), (1, 4)), (0, 1, 8, 2.0)),
    }


def reference(queries, latent, rope_key, key_weight, value_weight, log_sums, attn_out, out_grad):
    tok_count = queries.shape[0]
    head_width = NOPE + ROPE
    score_scale = head_width ** -0.5
    key_nope = jnp.dot(latent, key_weight, preferred_element_type=jnp.float32).astype(jnp.bfloat16)
    values = jnp.dot(latent, value_weight, preferred_element_type=jnp.float32).astype(jnp.bfloat16)
    query_heads = queries.reshape(tok_count, HEADS, head_width).transpose(1, 0, 2)
    key_heads = key_nope.reshape(tok_count, HEADS, NOPE).transpose(1, 0, 2)
    value_heads = values.reshape(tok_count, HEADS, VDIM).transpose(1, 0, 2)
    grad_heads = out_grad.reshape(tok_count, HEADS, VDIM).transpose(1, 0, 2)
    out_heads = attn_out.reshape(tok_count, HEADS, VDIM).transpose(1, 0, 2)
    row_terms = jnp.sum(out_heads.astype(jnp.float32) * grad_heads.astype(jnp.float32), axis=-1)
    positions = jnp.arange(tok_count, dtype=jnp.int32)
    causal = positions[None, :] <= positions[:, None]

    def one_head(operands):
        query_h, key_h, value_h, grad_h, lse_h, delta_h = operands
        scores = score_scale * (jnp.dot(query_h[:, :NOPE], key_h.T, preferred_element_type=jnp.float32)
                                + jnp.dot(query_h[:, NOPE:], rope_key.T, preferred_element_type=jnp.float32))
        attn_probs = jnp.exp(jnp.where(causal, scores - lse_h[:, None], -1e30))
        probs_b = attn_probs.astype(jnp.bfloat16)
        value_grad = jnp.dot(probs_b.T, grad_h, preferred_element_type=jnp.float32)
        prob_grad = jnp.dot(grad_h, value_h.T, preferred_element_type=jnp.float32)
        score_grad = (attn_probs * (prob_grad - delta_h[:, None])).astype(jnp.bfloat16)
        query_grad = score_scale * jnp.concatenate(
            [jnp.dot(score_grad, key_h, preferred_element_type=jnp.float32),
             jnp.dot(score_grad, rope_key, preferred_element_type=jnp.float32)], axis=1)
        key_grad = score_scale * jnp.dot(score_grad.T, query_h[:, :NOPE], preferred_element_type=jnp.float32)
        rope_grad = score_scale * jnp.dot(score_grad.T, query_h[:, NOPE:], preferred_element_type=jnp.float32)
        return query_grad, key_grad, rope_grad, value_grad

    query_grad, key_grad, rope_grad, value_grad = lax.map(
        one_head, (query_heads, key_heads, value_heads, grad_heads, log_sums, row_terms))
    d_queries = query_grad.transpose(1, 0, 2).reshape(tok_count, HEADS * head_width).astype(jnp.bfloat16)
    key_grad_b = key_grad.transpose(1, 0, 2).reshape(tok_count, HEADS * NOPE).astype(jnp.bfloat16)
    value_grad_b = value_grad.transpose(1, 0, 2).reshape(tok_count, HEADS * VDIM).astype(jnp.bfloat16)
    d_latent = (jnp.dot(key_grad_b, key_weight.T, preferred_element_type=jnp.float32)
                + jnp.dot(value_grad_b, value_weight.T, preferred_element_type=jnp.float32))
    d_rope = jnp.sum(rope_grad, axis=0)
    d_value_weight = jnp.dot(latent.T, value_grad_b, preferred_element_type=jnp.float32)
    return (d_queries, d_latent, d_rope, d_value_weight)
```

```python
import functools

import jax
import jax.numpy as jnp
from jax import lax
from jax.experimental import pallas as pl
from jax.experimental.pallas import tpu as pltpu
from jax.sharding import PartitionSpec as P

NOPE = 128
ROPE = 64
VDIM = 128
WIDE = 256
LOG2E = 1.4426950408889634
BF16 = jnp.bfloat16
F32 = jnp.float32
MESH = pl.DeviceIdType.MESH


def dot_nn(a, b):
    return lax.dot_general(a, b, (((1,), (0,)), ((), ())), preferred_element_type=F32)


def dot_nt(a, b):
    return lax.dot_general(a, b, (((1,), (1,)), ((), ())), preferred_element_type=F32)


def fused_kernel(
    ns,
    tp,
    heads,
    latent_dim,
    q_hbm,
    g_hbm,
    ao_hbm,
    lse_ref,
    latp_hbm,
    wk_hbm,
    wv_hbm,
    dq_ref,
    dlat_hbm,
    dvw_ref,
    q_v,
    g_v,
    ao_v,
    wk_v,
    wv_v,
    qs_s,
    qt_s,
    gt_s,
    dqt_s,
    delta_s,
    kc_s,
    kct_s,
    v_s,
    dk_s,
    dv_s,
    dvw_acc,
    dvw_b,
    dvw_rx,
    lat_all,
    crx,
    yrx,
    orx,
    own_acc,
    fin,
    ld,
    zr,
    zs,
    ds_,
    xr,
    xs,
    car,
    cas,
    cbr,
    cbs,
    r1r,
    r1s,
    yr,
    ys,
    orr,
    ors,
    dvr,
    dvs,
    agr,
    ags,
    acr,
    acs,
):
    i = lax.axis_index("sp")
    t = lax.axis_index("tp")
    ny = tp // 2
    nz = ns // 2
    z, x = i // 2, i % 2
    y, c = t // 2, t % 2
    rows, width = q_v.shape[0], NOPE + ROPE
    half, quart, piece = rows // 2, rows // 4, rows // tp
    scale = width ** (-0.5)
    lrows = latent_dim // ns

    first = 1 - x
    last = 2 * z + 1

    def block_of(n):
        return last - n

    my_half = pl.multiple_of(c * half, half)
    peer_half = pl.multiple_of((1 - c) * half, half)
    my_q = pl.multiple_of(c * half + x * quart, quart)
    other_q = pl.multiple_of(c * half + (1 - x) * quart, quart)
    core_peer = {"sp": i, "tp": y * 2 + 1 - c}
    x_peer = {"sp": 2 * z + 1 - x, "tp": t}

    def remote(src, dst, ssem, rsem, dev):
        return pltpu.make_async_remote_copy(
            src_ref=src, dst_ref=dst, send_sem=ssem, recv_sem=rsem, device_id=dev, device_id_type=MESH
        )

    def lat_rows(j, at, size):
        return lat_all.at[j, pl.ds(at, size)]

    own_cp = pltpu.make_async_copy(latp_hbm, lat_all.at[i], ld.at[0])
    own_cp.start()
    loads = [
        pltpu.make_async_copy(s, d, ld.at[k + 1])
        for k, (s, d) in enumerate(
            ((wk_hbm, wk_v), (wv_hbm, wv_v), (q_hbm, q_v), (g_hbm, g_v), (ao_hbm, ao_v))
        )
    ]
    for cp in loads:
        cp.start()

    barrier = pltpu.get_barrier_semaphore()
    for d in range(1, ns):
        pl.semaphore_signal(
            barrier, inc=1, device_id={"sp": (i + d) % ns, "tp": t}, device_id_type=MESH
        )
    for d in range(1, tp):
        pl.semaphore_signal(
            barrier, inc=1, device_id={"sp": i, "tp": (t + d) % tp}, device_id_type=MESH
        )
    pl.semaphore_wait(barrier, ns - 1 + tp - 1)
    own_cp.wait()

    def z_copy(j):
        return remote(
            lat_rows(j, my_q, quart), lat_rows(j, my_q, quart), zs.at[j], zr.at[j],
            {"sp": lax.min(i + 2, ns - 1), "tp": t},
        )

    def diag_copy():
        return remote(
            lat_rows(i, other_q, quart), lat_rows(i, other_q, quart), ds_.at[0], zr.at[i],
            {"sp": lax.min(2 * z + 3 - x, ns - 1), "tp": t},
        )

    def x_copy(j):
        return remote(
            lat_rows(j, my_q, quart), lat_rows(j, my_q, quart), xs.at[j], xr.at[j], x_peer
        )

    def x_wait(j):
        return remote(
            lat_rows(j, other_q, quart), lat_rows(j, other_q, quart), xs.at[j], xr.at[j], x_peer
        )

    def xh_copy(j):
        return remote(
            lat_rows(j, my_half, half), lat_rows(j, my_half, half), xs.at[j], xr.at[j], x_peer
        )

    def ca_copy(j):
        return remote(
            lat_rows(j, my_q, quart), lat_rows(j, my_q, quart), cas.at[j], car.at[j], core_peer
        )

    def cb_copy(j):
        return remote(
            lat_rows(j, other_q, quart), lat_rows(j, other_q, quart), cbs.at[j], cbr.at[j], core_peer
        )

    def ch_copy(j):
        return remote(
            lat_rows(j, my_half, half), lat_rows(j, my_half, half), cbs.at[j], cbr.at[j], core_peer
        )

    has_next = z + 1 < nz

    @pl.when(has_next)
    def _():
        z_copy(i).start()
        diag_copy().start()

    @pl.when(x == 0)
    def _():
        xh_copy(i).start()

    def stage_a(n):
        @pl.when(jnp.logical_and(n >= 2, n <= last))
        def _():
            j = block_of(n)
            z_copy(j).wait_recv()
            x_copy(j).start()
            ca_copy(j).start()

            @pl.when(has_next)
            def _():
                z_copy(j).start()

    def stage_b(n):
        j = block_of(n)

        @pl.when(jnp.logical_and(n == 1, x == 1))
        def _():
            xh_copy(j).wait_recv()
            ch_copy(j).start()

        @pl.when(jnp.logical_and(n >= 2, n <= last))
        def _():
            x_wait(j).wait_recv()
            cb_copy(j).start()

    def stage_c(n):
        j = block_of(n)

        @pl.when(jnp.logical_and(n == 1, x == 1))
        def _():
            ch_copy(j).wait_recv()

        @pl.when(n >= 2)
        def _():
            ca_copy(j).wait_recv()
            cb_copy(j).wait_recv()

    def sends_done(n):
        j = block_of(n)

        @pl.when(n == first)
        def _():
            @pl.when(has_next)
            def _():
                z_copy(i).wait_send()
                diag_copy().wait_send()

            @pl.when(x == 0)
            def _():
                xh_copy(i).wait_send()

        @pl.when(jnp.logical_and(n == 1, x == 1))
        def _():
            ch_copy(j).wait_send()

        @pl.when(n >= 2)
        def _():
            x_copy(j).wait_send()
            ca_copy(j).wait_send()
            cb_copy(j).wait_send()

            @pl.when(has_next)
            def _():
                z_copy(j).wait_send()

    def r1_copy(j):
        return remote(
            lat_rows(j + 1, peer_half, half), crx.at[j], r1s.at[j], r1r.at[j], core_peer
        )

    def y_copy(j, d):
        yy = (y + d) % ny
        at = pl.multiple_of(c * half + yy * piece, piece)
        return remote(
            lat_rows(j + 1, at, piece), yrx.at[j, d - 1], ys.at[j, d - 1], yr.at[j, d - 1],
            {"sp": i, "tp": yy * 2 + c},
        )

    my_piece = pl.multiple_of(c * half + y * piece, piece)

    def o_copy(j):
        return remote(
            lat_rows(j + 1, my_piece, piece), orx.at[i], ors.at[j], orr.at[i], {"sp": j, "tp": t}
        )

    def o_wait(src):
        return remote(
            lat_rows(i + 1, my_piece, piece), orx.at[src], ors.at[i], orr.at[src], {"sp": src, "tp": t}
        )

    def stage_r2(n):
        j = block_of(n)
        r1_copy(j).wait_recv()
        mine = lat_all[j + 1, pl.ds(my_half, half), :].astype(F32)
        lat_all[j + 1, pl.ds(my_half, half), :] = (mine + crx[j].astype(F32)).astype(BF16)
        for d in range(1, ny):
            y_copy(j, d).start()

    def stage_r3(n):
        j = block_of(n)
        total = lat_all[j + 1, pl.ds(my_piece, piece), :].astype(F32)
        for d in range(1, ny):
            y_copy(j, d).wait_recv()
            total = total + yrx[j, d - 1].astype(F32)
        for d in range(1, ny):
            y_copy(j, d).wait_send()
        r1_copy(j).wait_send()

        @pl.when(n == first)
        def _():
            own_acc[...] = total

        @pl.when(n > first)
        def _():
            lat_all[j + 1, pl.ds(my_piece, piece), :] = total.astype(BF16)
            o_copy(j).start()

    for cp in loads:
        cp.wait()
    for h in range(heads):
        qh = jnp.concatenate(
            [q_v[:, h * width : (h + 1) * width], jnp.zeros((rows, WIDE - width), BF16)], axis=1
        )
        qs_s[h] = qh
        qt_s[h] = qh.T
        gt = g_v[:, h * VDIM : (h + 1) * VDIM].T
        gt_s[h] = gt
        at = ao_v[:, h * VDIM : (h + 1) * VDIM].T
        delta_s[h : h + 1, :] = jnp.sum(gt.astype(F32) * at.astype(F32), axis=0, keepdims=True)
    dqt_s[...] = jnp.zeros_like(dqt_s)
    dvw_acc[...] = jnp.zeros_like(dvw_acc)

    def slot(n, carry):
        j = block_of(n)
        stage_c(n)
        rope = lat_all[j, :, latent_dim:]
        keys = dot_nn(lat_all[j, :, :latent_dim], wk_v[...]).astype(BF16)
        v_s[...] = dot_nn(lat_all[j, :, :latent_dim], wv_v[...]).astype(BF16)
        for h in range(heads):
            kc = jnp.concatenate([keys[:, h * NOPE : (h + 1) * NOPE], rope], axis=1)
            kc_s[h] = kc
            kct_s[h] = kc.T
        rope_sum = jnp.zeros((rows, WIDE - NOPE), F32)
        k_pos = lax.broadcasted_iota(jnp.int32, (rows, rows), 0)
        q_pos = lax.broadcasted_iota(jnp.int32, (rows, rows), 1)
        causal = k_pos - q_pos <= (i - j) * rows
        for h in range(heads):
            s = dot_nn(kc_s[h], qt_s[h])
            zz = s * (scale * LOG2E) - lse_ref[h : h + 1, :] * LOG2E
            p = jnp.exp2(jnp.where(causal, zz, -1e30))
            dp = dot_nn(v_s[:, h * VDIM : (h + 1) * VDIM], gt_s[h])
            ds = (p * (dp - delta_s[h : h + 1, :])).astype(BF16)
            dv_s[:, h * VDIM : (h + 1) * VDIM] = dot_nn(
                p.astype(BF16), g_v[:, h * VDIM : (h + 1) * VDIM]
            ).astype(BF16)
            dk = scale * dot_nn(ds, qs_s[h])
            dk_s[:, h * NOPE : (h + 1) * NOPE] = dk[:, :NOPE].astype(BF16)
            rope_sum = rope_sum + dk[:, NOPE:]
            dqt_s[h] += dot_nn(kct_s[h], ds)
            if h == 0:

                @pl.when(n > first)
                def _():
                    stage_r2(n - 1)

            if h == heads // 2:

                @pl.when(n > first + 1)
                def _():
                    stage_r3(n - 2)

        @pl.when(n > first)
        def _():
            stage_b(n + 1)
            sends_done(n - 1)

        dlat = dot_nt(dk_s[...], wk_v[...]) + dot_nt(dv_s[...], wv_v[...])
        lat_all[j + 1, :, :latent_dim] = dlat.astype(BF16)
        lat_all[j + 1, :, latent_dim:] = rope_sum.astype(BF16)
        r1_copy(j).start()
        dvw_acc[...] += dot_nn(lat_all[j, :, :latent_dim].T, dv_s[...])

        @pl.when(n == first)
        def _():
            stage_a(jnp.int32(2))

            @pl.when(x == 0)
            def _():
                stage_a(jnp.int32(3))

        stage_a(n + 3)

        @pl.when(n == first)
        def _():
            stage_b(n + 1)

        return carry

    lax.fori_loop(first, last + 1, slot, 0)

    def dv_copy(d):
        k = (i + d) % ns
        return remote(
            dvw_b.at[k], dvw_rx.at[ns - d], dvs.at[d], dvr.at[ns - d], {"sp": k, "tp": t}
        )

    def dv_wait(d):
        k = (i + d) % ns
        return remote(dvw_b.at[k], dvw_rx.at[d], dvs.at[d], dvr.at[d], {"sp": k, "tp": t})

    for k in range(ns):
        dvw_b[k] = dvw_acc[k * lrows : (k + 1) * lrows, :].astype(BF16)
    for d in range(1, ns):
        dv_copy(d).start()

    stage_r2(last)

    @pl.when(last > first)
    def _():
        stage_r3(last - 1)

    for h in range(heads):
        dq_ref[:, h * width : (h + 1) * width] = (scale * dqt_s[h]).T[:, :width].astype(BF16)

    stage_r3(last)

    dvw = dvw_acc[pl.ds(pl.multiple_of(i * lrows, lrows), lrows), :]
    for d in range(1, ns):
        dv_wait(d).wait_recv()
        dvw = dvw + dvw_rx[d].astype(F32)
    dvw_ref[...] = dvw

    def add(k, carry):
        o_wait(k).wait_recv()
        own_acc[...] += orx[k].astype(F32)
        return carry

    lax.fori_loop(i + 1, ns, add, 0)
    fin[pl.ds(my_piece, piece), :] = own_acc[...].astype(BF16)

    def ag_y(d):
        yy = (y + d) % ny
        return remote(
            fin.at[pl.ds(my_piece, piece)], fin.at[pl.ds(my_piece, piece)], ags.at[d - 1], agr.at[d - 1],
            {"sp": i, "tp": yy * 2 + c},
        )

    def ag_y_wait(d):
        at = pl.multiple_of(c * half + ((y + ny - d) % ny) * piece, piece)
        return remote(
            fin.at[pl.ds(at, piece)], fin.at[pl.ds(at, piece)], ags.at[d - 1], agr.at[d - 1],
            {"sp": i, "tp": ((y + ny - d) % ny) * 2 + c},
        )

    for d in range(1, ny):
        ag_y(d).start()
    for d in range(1, ny):
        ag_y_wait(d).wait_recv()
    ag_c = remote(
        fin.at[pl.ds(my_half, half)], fin.at[pl.ds(my_half, half)], acs.at[0], acr.at[0], core_peer
    )
    ag_c_wait = remote(
        fin.at[pl.ds(peer_half, half)], fin.at[pl.ds(peer_half, half)], acs.at[0], acr.at[0], core_peer
    )
    ag_c.start()

    sends_done(last)

    def drain(n, carry):
        o_copy(block_of(n)).wait_send()
        return carry

    lax.fori_loop(first + 1, last + 1, drain, 0)
    for d in range(1, ns):
        dv_copy(d).wait_send()
    for d in range(1, ny):
        ag_y(d).wait_send()
    ag_c_wait.wait_recv()
    ag_c.wait_send()
    out = pltpu.make_async_copy(fin, dlat_hbm, ld.at[0])
    out.start()
    out.wait()


def fused_backward(ns, tp, queries, out_grad, attn_out, lse, latp, key_weight, value_weight):
    rows = queries.shape[0]
    latent_dim, hv = key_weight.shape
    heads = hv // NOPE
    packed = latp.shape[1]
    lrows = latent_dim // ns
    ny = tp // 2
    hbm = pl.BlockSpec(memory_space=pl.ANY)
    vmem = pl.BlockSpec(memory_space=pltpu.VMEM)
    dma = pltpu.SemaphoreType.DMA
    return pl.pallas_call(
        functools.partial(fused_kernel, ns, tp, heads, latent_dim),
        in_specs=[hbm, hbm, hbm, vmem, hbm, hbm, hbm],
        out_specs=[vmem, hbm, vmem],
        out_shape=[
            jax.ShapeDtypeStruct(queries.shape, BF16),
            jax.ShapeDtypeStruct((rows, packed), BF16),
            jax.ShapeDtypeStruct((lrows, hv), F32),
        ],
        scratch_shapes=[
            pltpu.VMEM(queries.shape, BF16),
            pltpu.VMEM(out_grad.shape, BF16),
            pltpu.VMEM(attn_out.shape, BF16),
            pltpu.VMEM(key_weight.shape, BF16),
            pltpu.VMEM(value_weight.shape, BF16),
            pltpu.VMEM((heads, rows, WIDE), BF16),
            pltpu.VMEM((heads, WIDE, rows), BF16),
            pltpu.VMEM((heads, VDIM, rows), BF16),
            pltpu.VMEM((heads, WIDE, rows), F32),
            pltpu.VMEM((heads, rows), F32),
            pltpu.VMEM((heads, rows, WIDE), BF16),
            pltpu.VMEM((heads, WIDE, rows), BF16),
            pltpu.VMEM((rows, hv), BF16),
            pltpu.VMEM((rows, hv), BF16),
            pltpu.VMEM((rows, hv), BF16),
            pltpu.VMEM((latent_dim, hv), F32),
            pltpu.VMEM((ns, lrows, hv), BF16),
            pltpu.VMEM((ns, lrows, hv), BF16),
            pltpu.VMEM((ns + 1, rows, packed), BF16),
            pltpu.VMEM((ns, rows // 2, packed), BF16),
            pltpu.VMEM((ns, max(ny - 1, 1), rows // tp, packed), BF16),
            pltpu.VMEM((ns, rows // tp, packed), BF16),
            pltpu.VMEM((rows // tp, packed), F32),
            pltpu.VMEM((rows, packed), BF16),
            dma((6,)),
            dma((ns,)),
            dma((ns,)),
            dma((1,)),
            dma((ns,)),
            dma((ns,)),
            dma((ns,)),
            dma((ns,)),
            dma((ns,)),
            dma((ns,)),
            dma((ns,)),
            dma((ns,)),
            dma((ns, max(ny - 1, 1))),
            dma((ns, max(ny - 1, 1))),
            dma((ns,)),
            dma((ns,)),
            dma((ns,)),
            dma((ns,)),
            dma((max(ny - 1, 1),)),
            dma((max(ny - 1, 1),)),
            dma((1,)),
            dma((1,)),
        ],
        compiler_params=pltpu.CompilerParams(
            collective_id=0, has_side_effects=True, vmem_limit_bytes=67043328
        ),
    )(queries, out_grad, attn_out, lse, latp, key_weight, value_weight)


def per_device(queries, latent, rope_key, key_weight, value_weight, log_sums, attn_out, out_grad):
    rows, latent_dim = latent.shape
    latp = jnp.concatenate(
        [latent, rope_key, jnp.zeros((rows, WIDE - NOPE - ROPE), BF16)], axis=1
    )
    d_queries, dlat, d_value_weight = fused_backward(
        lax.axis_size("sp"), lax.axis_size("tp"),
        queries, out_grad, attn_out, log_sums, latp, key_weight, value_weight,
    )
    d_latent = dlat[:, :latent_dim].astype(F32)
    d_rope = dlat[:, latent_dim : latent_dim + ROPE].astype(F32)
    return (d_queries, d_latent, d_rope, d_value_weight)


def solution(mesh):
    placed = (
        P("sp", "tp"),
        P("sp", None),
        P("sp", None),
        P(None, "tp"),
        P(None, "tp"),
        P("tp", "sp"),
        P("sp", "tp"),
        P("sp", "tp"),
    )
    return jax.shard_map(
        per_device,
        mesh=mesh,
        in_specs=placed,
        out_specs=(P("sp", "tp"), P("sp", None), P("sp", None), P("sp", "tp")),
        check_vma=False,
    )
```

```python
import functools

import jax
import jax.numpy as jnp
from jax import lax
from jax.experimental import pallas as pl
from jax.experimental.pallas import tpu as pltpu
from jax.sharding import PartitionSpec as P

NOPE = 128
ROPE = 64
VDIM = 128
WIDE = 256
LOG2E = 1.4426950408889634
BF16 = jnp.bfloat16
F32 = jnp.float32
MESH = pl.DeviceIdType.MESH


def dot_nn(a, b):
    return lax.dot_general(a, b, (((1,), (0,)), ((), ())), preferred_element_type=F32)


def dot_nt(a, b):
    return lax.dot_general(a, b, (((1,), (1,)), ((), ())), preferred_element_type=F32)


def fused_kernel(
    ns,
    tp,
    heads,
    latent_dim,
    q_hbm,
    g_hbm,
    ao_hbm,
    lse_ref,
    lat_hbm,
    rope_hbm,
    wk_hbm,
    wv_hbm,
    dq_ref,
    dlat_hbm,
    drope_hbm,
    dvw_ref,
    q_v,
    g_v,
    ao_v,
    wk_v,
    wv_v,
    qs_s,
    qt_s,
    gt_s,
    dqt_s,
    delta_s,
    kc_s,
    kct_s,
    v_s,
    dk_s,
    dv_s,
    dvw_acc,
    dvw_b,
    dvw_rx,
    lat_all,
    crx,
    yrx,
    xrx,
    orx,
    own_acc,
    fin,
    ld,
    zr,
    zs,
    xr,
    xs,
    cr,
    cs,
    xrr,
    xrs,
    r1r,
    r1s,
    yr,
    ys,
    orr,
    ors,
    dvr,
    dvs,
    agr,
    ags,
    acr,
    acs,
):
    i = lax.axis_index("sp")
    t = lax.axis_index("tp")
    ny = tp // 2
    nz = ns // 2
    z, x = i // 2, i % 2
    y, c = t // 2, t % 2
    rows, width = q_v.shape[0], NOPE + ROPE
    half, quart, piece = rows // 2, rows // 4, rows // tp
    scale = width ** (-0.5)
    lrows = latent_dim // ns

    lower = 2 * z
    last = lower + x

    def block_of(n):
        down = 2 * (z - 1 - (n - 1) // 2) + (x + n - 1) % 2
        return lax.select(n == 0, i, lax.select(n > lower, jnp.int32(2 * z), down))

    def part_of(n):
        return lax.select(n == 0, jnp.int32(ns), lax.select(n == 1, jnp.int32(ns + 1), block_of(n - 1)))

    def own_column(n):
        return jnp.logical_and(n % 2 == 1, n <= lower)

    def other_column(n):
        return jnp.logical_and(n >= 1, jnp.logical_or(n % 2 == 0, n > lower))

    my_half = pl.multiple_of(c * half, half)
    peer_half = pl.multiple_of((1 - c) * half, half)
    core_peer = {"sp": i, "tp": y * 2 + 1 - c}
    x_peer = {"sp": 2 * z + 1 - x, "tp": t}
    above = {"sp": lax.min(i + 2, ns - 1), "tp": t}

    def remote(src, dst, ssem, rsem, dev):
        return pltpu.make_async_remote_copy(
            src_ref=src, dst_ref=dst, send_sem=ssem, recv_sem=rsem, device_id=dev, device_id_type=MESH
        )

    def lat_rows(j, at, size):
        return lat_all.at[j, pl.ds(at, size)]

    own_cps = [
        pltpu.make_async_copy(lat_hbm, lat_all.at[i, :, pl.ds(0, latent_dim)], ld.at[0]),
        pltpu.make_async_copy(rope_hbm, lat_all.at[i, :, pl.ds(latent_dim, WIDE - NOPE)], ld.at[6]),
    ]
    loads = [
        pltpu.make_async_copy(s, d, ld.at[k + 1])
        for k, (s, d) in enumerate(
            ((g_hbm, g_v), (q_hbm, q_v), (ao_hbm, ao_v), (wk_hbm, wk_v), (wv_hbm, wv_v))
        )
    ]
    for cp in own_cps + loads:
        cp.start()

    barrier = pltpu.get_barrier_semaphore()
    for d in range(1, ns):
        pl.semaphore_signal(
            barrier, inc=1, device_id={"sp": (i + d) % ns, "tp": t}, device_id_type=MESH
        )
    for d in range(1, tp):
        pl.semaphore_signal(
            barrier, inc=1, device_id={"sp": i, "tp": (t + d) % tp}, device_id_type=MESH
        )
    pl.semaphore_wait(barrier, ns - 1 + tp - 1)
    for cp in own_cps:
        cp.wait()

    def quarter(j, k):
        return lat_rows(j, pl.multiple_of(c * half + k * quart, quart), quart)

    def z_copy(j, k):
        return remote(quarter(j, k), quarter(j, k), zs.at[j, k], zr.at[j, k], above)

    def x_copy(j, k):
        return remote(quarter(j, k), quarter(j, k), xs.at[j, k], xr.at[j, k], x_peer)

    def c_copy(j):
        return remote(lat_rows(j, my_half, half), lat_rows(j, my_half, half), cs.at[j], cr.at[j], core_peer)

    has_next = z + 1 < nz

    @pl.when(has_next)
    def _():
        z_copy(i, 0).start()
        z_copy(i, 1).start()

    @pl.when(x == 0)
    def _():
        x_copy(i, 0).start()

    def stage_a(n, k):
        @pl.when(own_column(n))
        def _():
            j = block_of(n)
            z_copy(j, k).wait_recv()
            x_copy(j, k).start()

            @pl.when(has_next)
            def _():
                z_copy(j, k).start()

            if k == 1:
                c_copy(j).start()

    def stage_b(n):
        @pl.when(jnp.logical_and(other_column(n), n <= last))
        def _():
            j = block_of(n)
            x_copy(j, 0).wait_recv()
            x_copy(j, 1).wait_recv()
            c_copy(j).start()

    def sends_done(n):
        j = block_of(n)
        c_copy(j).wait_send()

        @pl.when(own_column(n))
        def _():
            for k in range(2):
                x_copy(j, k).wait_send()

            @pl.when(has_next)
            def _():
                for k in range(2):
                    z_copy(j, k).wait_send()

    def r1_copy(n):
        j = block_of(n)
        return remote(
            lat_rows(part_of(n), peer_half, half), crx.at[j], r1s.at[j], r1r.at[j], core_peer
        )

    def y_copy(n, d):
        j = block_of(n)
        yy = (y + d) % ny
        at = pl.multiple_of(c * half + yy * piece, piece)
        return remote(
            lat_rows(part_of(n), at, piece), yrx.at[j, d - 1], ys.at[j, d - 1], yr.at[j, d - 1],
            {"sp": i, "tp": yy * 2 + c},
        )

    my_piece = pl.multiple_of(c * half + y * piece, piece)

    def xr_copy(n):
        j = block_of(n)
        return remote(lat_rows(part_of(n), my_piece, piece), xrx.at[j], xrs.at[j], xrr.at[j], x_peer)

    def o_copy(n):
        j = block_of(n)
        return remote(
            lat_rows(part_of(n), my_piece, piece), orx.at[z], ors.at[j], orr.at[z], {"sp": j, "tp": t}
        )

    def o_wait(zz):
        return remote(
            lat_rows(i, my_piece, piece), orx.at[zz], ors.at[i], orr.at[zz], x_peer
        )

    def stage_r2(n):
        j = block_of(n)
        b = part_of(n)
        r1_copy(n).wait_recv()
        mine = lat_all[b, pl.ds(my_half, half), :].astype(F32)
        lat_all[b, pl.ds(my_half, half), :] = (mine + crx[j].astype(F32)).astype(BF16)
        for d in range(1, ny):
            y_copy(n, d).start()

    def stage_r3(n):
        j = block_of(n)
        b = part_of(n)
        total = lat_all[b, pl.ds(my_piece, piece), :].astype(F32)
        for d in range(1, ny):
            y_copy(n, d).wait_recv()
            total = total + yrx[j, d - 1].astype(F32)
        for d in range(1, ny):
            y_copy(n, d).wait_send()
        r1_copy(n).wait_send()

        @pl.when(n == 0)
        def _():
            own_acc[...] = total

        @pl.when(n > 0)
        def _():
            lat_all[b, pl.ds(my_piece, piece), :] = total.astype(BF16)

        @pl.when(jnp.logical_and(other_column(n), n <= lower))
        def _():
            xr_copy(n).start()

        @pl.when(n > lower)
        def _():
            @pl.when(n > 0)
            def _():
                o_copy(n).start()

    def stage_r4(n):
        @pl.when(own_column(n))
        def _():
            j = block_of(n)
            b = part_of(n)
            xr_copy(n).wait_recv()
            total = lat_all[b, pl.ds(my_piece, piece), :].astype(F32) + xrx[j].astype(F32)
            lat_all[b, pl.ds(my_piece, piece), :] = total.astype(BF16)
            o_copy(n).start()

    for cp in loads:
        cp.wait()
    for h in range(heads):
        qh = jnp.concatenate(
            [q_v[:, h * width : (h + 1) * width], jnp.zeros((rows, WIDE - width), BF16)], axis=1
        )
        qs_s[h] = qh
        qt_s[h] = qh.T
        gt = g_v[:, h * VDIM : (h + 1) * VDIM].T
        gt_s[h] = gt
        at = ao_v[:, h * VDIM : (h + 1) * VDIM].T
        delta_s[h : h + 1, :] = jnp.sum(gt.astype(F32) * at.astype(F32), axis=0, keepdims=True)
    dqt_s[...] = jnp.zeros_like(dqt_s)
    dvw_acc[...] = jnp.zeros_like(dvw_acc)

    def slot(n, carry):
        j = block_of(n)
        b = part_of(n)

        @pl.when(n > 0)
        def _():
            c_copy(j).wait_recv()

        rope = lat_all[j, :, latent_dim:]
        keys = dot_nn(lat_all[j, :, :latent_dim], wk_v[...]).astype(BF16)
        v_s[...] = dot_nn(lat_all[j, :, :latent_dim], wv_v[...]).astype(BF16)
        for h in range(heads):
            kc = jnp.concatenate([keys[:, h * NOPE : (h + 1) * NOPE], rope], axis=1)
            kc_s[h] = kc
            kct_s[h] = kc.T
        rope_sum = jnp.zeros((rows, WIDE - NOPE), F32)
        k_pos = lax.broadcasted_iota(jnp.int32, (rows, rows), 0)
        q_pos = lax.broadcasted_iota(jnp.int32, (rows, rows), 1)
        causal = k_pos - q_pos <= (i - j) * rows
        for h in range(heads):
            s = dot_nn(kc_s[h], qt_s[h])
            zz = s * (scale * LOG2E) - lse_ref[h : h + 1, :] * LOG2E
            p = jnp.exp2(jnp.where(causal, zz, -1e30))
            dp = dot_nn(v_s[:, h * VDIM : (h + 1) * VDIM], gt_s[h])
            ds = (p * (dp - delta_s[h : h + 1, :])).astype(BF16)
            dv_s[:, h * VDIM : (h + 1) * VDIM] = dot_nn(
                p.astype(BF16), g_v[:, h * VDIM : (h + 1) * VDIM]
            ).astype(BF16)
            dk = scale * dot_nn(ds, qs_s[h])
            dk_s[:, h * NOPE : (h + 1) * NOPE] = dk[:, :NOPE].astype(BF16)
            rope_sum = rope_sum + dk[:, NOPE:]
            dqt_s[h] += dot_nn(kct_s[h], ds)
            if h == 0:

                @pl.when(n > 0)
                def _():
                    stage_r2(n - 1)

            if h == (heads - 1) // 2:

                @pl.when(n > 1)
                def _():
                    stage_a(n + 1, 1)

            if h == heads // 2:

                @pl.when(n > 1)
                def _():
                    stage_r3(n - 2)

                @pl.when(n == 0)
                def _():
                    stage_a(n + 1, 0)

        @pl.when(n > 4)
        def _():
            stage_r4(n - 4)

        @pl.when(n > 1)
        def _():
            sends_done(n - 1)

        dlat = dot_nt(dk_s[...], wk_v[...]) + dot_nt(dv_s[...], wv_v[...])
        lat_all[b, :, :latent_dim] = dlat.astype(BF16)
        lat_all[b, :, latent_dim:] = rope_sum.astype(BF16)
        r1_copy(n).start()

        @pl.when(n == 0)
        def _():
            stage_a(n + 1, 1)

        stage_b(n + 1)
        dvw_acc[...] += dot_nn(lat_all[j, :, :latent_dim].T, dv_s[...])

        @pl.when(n > 0)
        def _():
            stage_a(n + 2, 0)

        @pl.when(jnp.logical_and(x == 0, n == lax.min(2, last)))
        def _():
            x_copy(i, 1).start()

        return carry

    lax.fori_loop(0, last + 1, slot, 0)

    def dv_copy(d):
        k = (i + d) % ns
        return remote(
            dvw_b.at[k], dvw_rx.at[ns - d], dvs.at[d], dvr.at[ns - d], {"sp": k, "tp": t}
        )

    def dv_wait(d):
        k = (i + d) % ns
        return remote(dvw_b.at[k], dvw_rx.at[d], dvs.at[d], dvr.at[d], {"sp": k, "tp": t})

    for k in range(ns):
        dvw_b[k] = dvw_acc[k * lrows : (k + 1) * lrows, :].astype(BF16)
    for d in range(1, ns):
        dv_copy(d).start()

    stage_r2(last)

    @pl.when(last > 3)
    def _():
        stage_r4(last - 3)

    @pl.when(last > 0)
    def _():
        stage_r3(last - 1)

    for h in range(heads):
        dq_ref[:, h * width : (h + 1) * width] = (scale * dqt_s[h]).T[:, :width].astype(BF16)

    stage_r3(last)

    def tail(n, carry):
        stage_r4(n)
        return carry

    lax.fori_loop(lax.max(last - 2, 1), lower + 1, tail, 0)

    dvw = dvw_acc[pl.ds(pl.multiple_of(i * lrows, lrows), lrows), :]
    for d in range(1, ns):
        dv_wait(d).wait_recv()
        dvw = dvw + dvw_rx[d].astype(F32)
    dvw_ref[...] = dvw

    def add(k, carry):
        o_wait(k).wait_recv()
        own_acc[...] += orx[k].astype(F32)
        return carry

    @pl.when(x == 0)
    def _():
        add(z, 0)

    lax.fori_loop(z + 1, nz, add, 0)
    fin[pl.ds(my_piece, piece), :] = own_acc[...].astype(BF16)

    def ag_y(d):
        yy = (y + d) % ny
        return remote(
            fin.at[pl.ds(my_piece, piece)], fin.at[pl.ds(my_piece, piece)], ags.at[d - 1], agr.at[d - 1],
            {"sp": i, "tp": yy * 2 + c},
        )

    def ag_y_wait(d):
        at = pl.multiple_of(c * half + ((y + ny - d) % ny) * piece, piece)
        return remote(
            fin.at[pl.ds(at, piece)], fin.at[pl.ds(at, piece)], ags.at[d - 1], agr.at[d - 1],
            {"sp": i, "tp": ((y + ny - d) % ny) * 2 + c},
        )

    for d in range(1, ny):
        ag_y(d).start()
    for d in range(1, ny):
        ag_y_wait(d).wait_recv()
    ag_c = remote(
        fin.at[pl.ds(my_half, half)], fin.at[pl.ds(my_half, half)], acs.at[0], acr.at[0], core_peer
    )
    ag_c_wait = remote(
        fin.at[pl.ds(peer_half, half)], fin.at[pl.ds(peer_half, half)], acs.at[0], acr.at[0], core_peer
    )
    ag_c.start()

    @pl.when(last > 0)
    def _():
        sends_done(last)

    @pl.when(has_next)
    def _():
        z_copy(i, 0).wait_send()
        z_copy(i, 1).wait_send()

    @pl.when(x == 0)
    def _():
        x_copy(i, 0).wait_send()
        x_copy(i, 1).wait_send()

    def drain(n, carry):
        @pl.when(jnp.logical_or(own_column(n), n > lower))
        def _():
            o_copy(n).wait_send()

        @pl.when(jnp.logical_and(other_column(n), n <= lower))
        def _():
            xr_copy(n).wait_send()

        return carry

    lax.fori_loop(1, last + 1, drain, 0)
    for d in range(1, ns):
        dv_copy(d).wait_send()
    for d in range(1, ny):
        ag_y(d).wait_send()
    ag_c_wait.wait_recv()
    ag_c.wait_send()
    outs = [
        pltpu.make_async_copy(fin.at[:, pl.ds(0, latent_dim)], dlat_hbm, ld.at[0]),
        pltpu.make_async_copy(fin.at[:, pl.ds(latent_dim, WIDE - NOPE)], drope_hbm, ld.at[6]),
    ]
    for out in outs:
        out.start()
    for out in outs:
        out.wait()


def fused_backward(ns, tp, queries, out_grad, attn_out, lse, latent, rope, key_weight, value_weight):
    rows = queries.shape[0]
    latent_dim, hv = key_weight.shape
    heads = hv // NOPE
    packed = latent_dim + rope.shape[1]
    lrows = latent_dim // ns
    ny = tp // 2
    hbm = pl.BlockSpec(memory_space=pl.ANY)
    vmem = pl.BlockSpec(memory_space=pltpu.VMEM)
    dma = pltpu.SemaphoreType.DMA
    return pl.pallas_call(
        functools.partial(fused_kernel, ns, tp, heads, latent_dim),
        in_specs=[hbm, hbm, hbm, vmem, hbm, hbm, hbm, hbm],
        out_specs=[vmem, hbm, hbm, vmem],
        out_shape=[
            jax.ShapeDtypeStruct(queries.shape, BF16),
            jax.ShapeDtypeStruct(latent.shape, BF16),
            jax.ShapeDtypeStruct(rope.shape, BF16),
            jax.ShapeDtypeStruct((lrows, hv), F32),
        ],
        scratch_shapes=[
            pltpu.VMEM(queries.shape, BF16),
            pltpu.VMEM(out_grad.shape, BF16),
            pltpu.VMEM(attn_out.shape, BF16),
            pltpu.VMEM(key_weight.shape, BF16),
            pltpu.VMEM(value_weight.shape, BF16),
            pltpu.VMEM((heads, rows, WIDE), BF16),
            pltpu.VMEM((heads, WIDE, rows), BF16),
            pltpu.VMEM((heads, VDIM, rows), BF16),
            pltpu.VMEM((heads, WIDE, rows), F32),
            pltpu.VMEM((heads, rows), F32),
            pltpu.VMEM((heads, rows, WIDE), BF16),
            pltpu.VMEM((heads, WIDE, rows), BF16),
            pltpu.VMEM((rows, hv), BF16),
            pltpu.VMEM((rows, hv), BF16),
            pltpu.VMEM((rows, hv), BF16),
            pltpu.VMEM((latent_dim, hv), F32),
            pltpu.VMEM((ns, lrows, hv), BF16),
            pltpu.VMEM((ns, lrows, hv), BF16),
            pltpu.VMEM((ns + 2, rows, packed), BF16),
            pltpu.VMEM((ns, rows // 2, packed), BF16),
            pltpu.VMEM((ns, max(ny - 1, 1), rows // tp, packed), BF16),
            pltpu.VMEM((ns, rows // tp, packed), BF16),
            pltpu.VMEM((ns // 2, rows // tp, packed), BF16),
            pltpu.VMEM((rows // tp, packed), F32),
            pltpu.VMEM((rows, packed), BF16),
            dma((7,)),
            dma((ns, 2)),
            dma((ns, 2)),
            dma((ns, 2)),
            dma((ns, 2)),
            dma((ns,)),
            dma((ns,)),
            dma((ns,)),
            dma((ns,)),
            dma((ns,)),
            dma((ns,)),
            dma((ns, max(ny - 1, 1))),
            dma((ns, max(ny - 1, 1))),
            dma((ns // 2,)),
            dma((ns,)),
            dma((ns,)),
            dma((ns,)),
            dma((max(ny - 1, 1),)),
            dma((max(ny - 1, 1),)),
            dma((1,)),
            dma((1,)),
        ],
        compiler_params=pltpu.CompilerParams(
            collective_id=0, has_side_effects=True, vmem_limit_bytes=67043328
        ),
    )(queries, out_grad, attn_out, lse, latent, rope, key_weight, value_weight)


def per_device(queries, latent, rope_key, key_weight, value_weight, log_sums, attn_out, out_grad):
    rope = jnp.pad(rope_key, ((0, 0), (0, WIDE - NOPE - ROPE)))
    d_queries, dlat, drope, d_value_weight = fused_backward(
        lax.axis_size("sp"), lax.axis_size("tp"),
        queries, out_grad, attn_out, log_sums, latent, rope, key_weight, value_weight,
    )
    d_latent = dlat.astype(F32)
    d_rope = drope[:, :ROPE].astype(F32)
    return (d_queries, d_latent, d_rope, d_value_weight)


def solution(mesh):
    placed = (
        P("sp", "tp"),
        P("sp", None),
        P("sp", None),
        P(None, "tp"),
        P(None, "tp"),
        P("tp", "sp"),
        P("sp", "tp"),
        P("sp", "tp"),
    )
    return jax.shard_map(
        per_device,
        mesh=mesh,
        in_specs=placed,
        out_specs=(P("sp", "tp"), P("sp", None), P("sp", None), P("sp", "tp")),
        check_vma=False,
    )
```

```python
import functools

import jax
import jax.numpy as jnp
from jax import lax
from jax.experimental import pallas as pl
from jax.experimental.pallas import tpu as pltpu
from jax.sharding import PartitionSpec as P

NOPE = 128
ROPE = 64
VDIM = 128
WIDE = 256
LOG2E = 1.4426950408889634
BF16 = jnp.bfloat16
F32 = jnp.float32
MESH = pl.DeviceIdType.MESH


def dot_nn(a, b):
    return lax.dot_general(a, b, (((1,), (0,)), ((), ())), preferred_element_type=F32)


def dot_nt(a, b):
    return lax.dot_general(a, b, (((1,), (1,)), ((), ())), preferred_element_type=F32)


def fused_kernel(
    ns,
    tp,
    heads,
    latent_dim,
    q_hbm,
    g_hbm,
    ao_hbm,
    lse_ref,
    lat_hbm,
    rope_hbm,
    wk_hbm,
    wv_hbm,
    dq_ref,
    dlat_hbm,
    drope_hbm,
    dvw_ref,
    q_v,
    g_v,
    fq_v,
    lse_s,
    ao_v,
    wk_v,
    wv_v,
    qs_s,
    qt_s,
    gt_s,
    dqt_s,
    delta_s,
    kc_s,
    kct_s,
    v_s,
    dk_s,
    dv_s,
    dvw_acc,
    dvw_b,
    dvw_rx,
    lat_all,
    crx,
    yrx,
    xrx,
    orx,
    own_acc,
    fin,
    ld,
    zr,
    zs,
    xr,
    xs,
    cr,
    cs,
    xrr,
    xrs,
    r1r,
    r1s,
    yr,
    ys,
    orr,
    ors,
    dvr,
    dvs,
    agr,
    ags,
    acr,
    acs,
    vr,
    vs,
):
    i = lax.axis_index("sp")
    t = lax.axis_index("tp")
    ny = tp // 2
    nz = ns // 2
    z, x = i // 2, i % 2
    y, c = t // 2, t % 2
    rows, width = q_v.shape[0], NOPE + ROPE
    half, quart, piece = rows // 2, rows // 4, rows // tp
    scale = width ** (-0.5)
    lrows = latent_dim // ns

    top = nz - 1
    is_top, is_low = z == top, z == 0
    lower = lax.select(is_top, 2 * (z - 1), 2 * z)
    base = lower + x
    last = base + lax.select(is_low, jnp.int32(2), jnp.int32(0))

    def visiting(n):
        return n > base

    def block_of(n):
        down = 2 * (z - 1 - (n - 1) // 2) + (x + n - 1) % 2
        home = lax.select(n == 0, i, lax.select(n > lower, jnp.int32(2 * z), down))
        return lax.select(visiting(n), lax.select(n == base + 1, i, 1 - i), home)

    def key_of(n):
        return lax.select(visiting(n), block_of(n) + 2, block_of(n))

    def part_of(n):
        later = lax.select(is_low, n, block_of(n - 1))
        return lax.select(n == 0, jnp.int32(ns), lax.select(n == 1, jnp.int32(ns + 1), later))

    def own_column(n):
        return jnp.logical_and(n % 2 == 1, n <= lower)

    def for_x_sum(n):
        return jnp.logical_and(jnp.logical_and(n >= 1, n <= lower), n % 2 == 0)

    def in_plane(n):
        return jnp.logical_and(x == 1, n == lower + 1)

    def by_x(n):
        mine = jnp.logical_and(is_low, jnp.logical_and(x == 0, n == base + 2))
        return jnp.logical_or(for_x_sum(n), jnp.logical_or(in_plane(n), mine))

    def visit_out(n):
        return jnp.logical_and(is_low, n == base + 2)

    my_half = pl.multiple_of(c * half, half)
    peer_half = pl.multiple_of((1 - c) * half, half)
    core_peer = {"sp": i, "tp": y * 2 + 1 - c}
    x_peer = {"sp": 2 * z + 1 - x, "tp": t}
    above = {"sp": lax.min(i + 2, ns - 1), "tp": t}

    def remote(src, dst, ssem, rsem, dev):
        return pltpu.make_async_remote_copy(
            src_ref=src, dst_ref=dst, send_sem=ssem, recv_sem=rsem, device_id=dev, device_id_type=MESH
        )

    def lat_rows(j, at, size):
        return lat_all.at[j, pl.ds(at, size)]

    own_cps = [
        pltpu.make_async_copy(lat_hbm, lat_all.at[i, :, pl.ds(0, latent_dim)], ld.at[0]),
        pltpu.make_async_copy(rope_hbm, lat_all.at[i, :, pl.ds(latent_dim, WIDE - NOPE)], ld.at[6]),
    ]
    loads = [
        pltpu.make_async_copy(s, d, ld.at[k + 1])
        for k, (s, d) in enumerate(
            ((g_hbm, g_v.at[0]), (q_hbm, q_v), (ao_hbm, ao_v), (wk_hbm, wk_v), (wv_hbm, wv_v))
        )
    ]
    for cp in own_cps + loads:
        cp.start()

    barrier = pltpu.get_barrier_semaphore()
    for d in range(1, ns):
        pl.semaphore_signal(
            barrier, inc=1, device_id={"sp": (i + d) % ns, "tp": t}, device_id_type=MESH
        )
    for d in range(1, tp):
        pl.semaphore_signal(
            barrier, inc=1, device_id={"sp": i, "tp": (t + d) % tp}, device_id_type=MESH
        )
    pl.semaphore_wait(barrier, ns - 1 + tp - 1)
    for cp in own_cps:
        cp.wait()

    def quarter(j, k):
        return lat_rows(j, pl.multiple_of(c * half + k * quart, quart), quart)

    def z_copy(j, k):
        return remote(quarter(j, k), quarter(j, k), zs.at[j, k], zr.at[j, k], above)

    def x_copy(j, k):
        return remote(quarter(j, k), quarter(j, k), xs.at[j, k], xr.at[j, k], x_peer)

    def c_copy(j):
        return remote(lat_rows(j, my_half, half), lat_rows(j, my_half, half), cs.at[j], cr.at[j], core_peer)

    has_next = z + 1 < nz

    @pl.when(has_next)
    def _():
        z_copy(i, 0).start()
        z_copy(i, 1).start()

    @pl.when(jnp.logical_or(x == 0, is_low))
    def _():
        x_copy(i, 0).start()

    @pl.when(is_low)
    def _():
        x_copy(i, 1).start()

    def goes_on(n):
        return jnp.logical_and(has_next, jnp.logical_or(z + 1 != top, block_of(n) >= 2))

    low_peer = {"sp": x, "tp": t}
    top_peer = {"sp": 2 * top + x, "tp": t}

    visits = ((g_v.at[0], g_v.at[1]), (q_v, fq_v), (lse_ref, lse_s.at[1]), (delta_s.at[0], delta_s.at[1]))

    def visit_copy(k):
        return remote(visits[k][0], visits[k][1], vs.at[k], vr.at[k], low_peer)

    def back_copy():
        return remote(fq_v, fq_v, vs.at[4], vr.at[4], top_peer)

    def stage_a(n, k):
        @pl.when(own_column(n))
        def _():
            j = block_of(n)
            z_copy(j, k).wait_recv()
            x_copy(j, k).start()

            @pl.when(goes_on(n))
            def _():
                z_copy(j, k).start()

            if k == 1:
                c_copy(j).start()

    def stage_b(n):
        @pl.when(by_x(n))
        def _():
            j = block_of(n)
            x_copy(j, 0).wait_recv()
            x_copy(j, 1).wait_recv()
            c_copy(j).start()

    def sends_done(n):
        j = block_of(n)

        @pl.when(jnp.logical_or(own_column(n), by_x(n)))
        def _():
            c_copy(j).wait_send()

        @pl.when(own_column(n))
        def _():
            for k in range(2):
                x_copy(j, k).wait_send()

            @pl.when(goes_on(n))
            def _():
                for k in range(2):
                    z_copy(j, k).wait_send()

    def r1_copy(n):
        j = key_of(n)
        return remote(
            lat_rows(part_of(n), peer_half, half), crx.at[j], r1s.at[j], r1r.at[j], core_peer
        )

    def y_copy(n, d):
        j = key_of(n)
        yy = (y + d) % ny
        at = pl.multiple_of(c * half + yy * piece, piece)
        return remote(
            lat_rows(part_of(n), at, piece), yrx.at[j, d - 1], ys.at[j, d - 1], yr.at[j, d - 1],
            {"sp": i, "tp": yy * 2 + c},
        )

    my_piece = pl.multiple_of(c * half + y * piece, piece)

    def xr_copy(n):
        j = block_of(n)
        return remote(lat_rows(part_of(n), my_piece, piece), xrx.at[j], xrs.at[j], xrr.at[j], x_peer)

    def o_copy(n):
        return remote(
            lat_rows(part_of(n), my_piece, piece), orx.at[z], ors.at[key_of(n)], orr.at[z],
            {"sp": block_of(n), "tp": t},
        )

    def v_copy(n):
        return remote(
            lat_rows(part_of(n), my_piece, piece), orx.at[nz], ors.at[key_of(n)], orr.at[nz], x_peer
        )

    def o_wait(zz):
        return remote(
            lat_rows(i, my_piece, piece), orx.at[zz], ors.at[i], orr.at[zz], x_peer
        )

    def stage_r2(n):
        j = key_of(n)
        b = part_of(n)
        r1_copy(n).wait_recv()
        mine = lat_all[b, pl.ds(my_half, half), :].astype(F32)
        lat_all[b, pl.ds(my_half, half), :] = (mine + crx[j].astype(F32)).astype(BF16)
        for d in range(1, ny):
            y_copy(n, d).start()

    def stage_r3(n):
        j = key_of(n)
        b = part_of(n)
        total = lat_all[b, pl.ds(my_piece, piece), :].astype(F32)
        for d in range(1, ny):
            y_copy(n, d).wait_recv()
            total = total + yrx[j, d - 1].astype(F32)
        for d in range(1, ny):
            y_copy(n, d).wait_send()
        r1_copy(n).wait_send()

        @pl.when(n == 0)
        def _():
            own_acc[...] = total

        @pl.when(jnp.logical_and(is_low, n == base + 1))
        def _():
            own_acc[...] += total

        @pl.when(n > 0)
        def _():
            lat_all[b, pl.ds(my_piece, piece), :] = total.astype(BF16)

        @pl.when(for_x_sum(n))
        def _():
            xr_copy(n).start()

        @pl.when(in_plane(n))
        def _():
            o_copy(n).start()

        @pl.when(visit_out(n))
        def _():
            v_copy(n).start()

    def stage_r4(n):
        @pl.when(own_column(n))
        def _():
            j = block_of(n)
            b = part_of(n)
            xr_copy(n).wait_recv()
            total = lat_all[b, pl.ds(my_piece, piece), :].astype(F32) + xrx[j].astype(F32)
            lat_all[b, pl.ds(my_piece, piece), :] = total.astype(BF16)
            o_copy(n).start()

    def prepare(qi, q_ref):
        for h in range(heads):
            qh = jnp.concatenate(
                [q_ref[:, h * width : (h + 1) * width], jnp.zeros((rows, WIDE - width), BF16)], axis=1
            )
            qs_s[qi, h] = qh
            qt_s[qi, h] = qh.T
            gt_s[qi, h] = g_v[qi, :, h * VDIM : (h + 1) * VDIM].T
        dqt_s[qi] = jnp.zeros_like(dqt_s[qi])

    for cp in loads[:2]:
        cp.wait()

    @pl.when(is_top)
    def _():
        for k in range(3):
            visit_copy(k).start()

    for cp in loads[2:]:
        cp.wait()
    prepare(0, q_v)
    for h in range(heads):
        at = ao_v[:, h * VDIM : (h + 1) * VDIM].T
        delta_s[0, h : h + 1, :] = jnp.sum(
            gt_s[0, h].astype(F32) * at.astype(F32), axis=0, keepdims=True
        )
    lse_s[0] = lse_ref[...]

    @pl.when(is_top)
    def _():
        visit_copy(3).start()

    dvw_acc[...] = jnp.zeros_like(dvw_acc)

    def slot(n, carry):
        j = block_of(n)
        b = part_of(n)
        qi = lax.select(visiting(n), jnp.int32(1), jnp.int32(0))
        q_block = lax.select(visiting(n), 2 * top + x, i)

        @pl.when(jnp.logical_or(own_column(n), by_x(n)))
        def _():
            c_copy(j).wait_recv()

        @pl.when(n == base + 1)
        def _():
            for k in range(4):
                visit_copy(k).wait_recv()
            prepare(1, fq_v)

        rope = lat_all[j, :, latent_dim:]
        keys = dot_nn(lat_all[j, :, :latent_dim], wk_v[...]).astype(BF16)
        v_s[...] = dot_nn(lat_all[j, :, :latent_dim], wv_v[...]).astype(BF16)
        for h in range(heads):
            kc = jnp.concatenate([keys[:, h * NOPE : (h + 1) * NOPE], rope], axis=1)
            kc_s[h] = kc
            kct_s[h] = kc.T
        rope_sum = jnp.zeros((rows, WIDE - NOPE), F32)
        k_pos = lax.broadcasted_iota(jnp.int32, (rows, rows), 0)
        q_pos = lax.broadcasted_iota(jnp.int32, (rows, rows), 1)
        causal = k_pos - q_pos <= (q_block - j) * rows
        for h in range(heads):
            s = dot_nn(kc_s[h], qt_s[qi, h])
            zz = s * (scale * LOG2E) - lse_s[qi, h : h + 1, :] * LOG2E
            p = jnp.exp2(jnp.where(causal, zz, -1e30))
            dp = dot_nn(v_s[:, h * VDIM : (h + 1) * VDIM], gt_s[qi, h])
            ds = (p * (dp - delta_s[qi, h : h + 1, :])).astype(BF16)
            dv_s[:, h * VDIM : (h + 1) * VDIM] = dot_nn(
                p.astype(BF16), g_v[qi, :, h * VDIM : (h + 1) * VDIM]
            ).astype(BF16)
            dk = scale * dot_nn(ds, qs_s[qi, h])
            dk_s[:, h * NOPE : (h + 1) * NOPE] = dk[:, :NOPE].astype(BF16)
            rope_sum = rope_sum + dk[:, NOPE:]
            dqt_s[qi, h] += dot_nn(kct_s[h], ds)
            if h == 0:

                @pl.when(n > 0)
                def _():
                    stage_r2(n - 1)

            if h == (heads - 1) // 2:

                @pl.when(n > 1)
                def _():
                    stage_a(n + 1, 1)

            if h == heads // 2:

                @pl.when(n > 1)
                def _():
                    stage_r3(n - 2)

                @pl.when(n == 0)
                def _():
                    stage_a(n + 1, 0)

        @pl.when(n > 4)
        def _():
            stage_r4(n - 4)

        @pl.when(n > 1)
        def _():
            sends_done(n - 1)

        dlat = dot_nt(dk_s[...], wk_v[...]) + dot_nt(dv_s[...], wv_v[...])
        lat_all[b, :, :latent_dim] = dlat.astype(BF16)
        lat_all[b, :, latent_dim:] = rope_sum.astype(BF16)
        r1_copy(n).start()

        @pl.when(n == 0)
        def _():
            stage_a(n + 1, 1)

        stage_b(n + 1)
        dvw_acc[...] += dot_nn(lat_all[j, :, :latent_dim].T, dv_s[...])

        @pl.when(n > 0)
        def _():
            stage_a(n + 2, 0)

        @pl.when(jnp.logical_and(jnp.logical_and(x == 0, z > 0), n == 2))
        def _():
            x_copy(i, 1).start()

        return carry

    lax.fori_loop(0, last + 1, slot, 0)

    @pl.when(is_low)
    def _():
        for h in range(heads):
            fq_v[:, h * width : (h + 1) * width] = (scale * dqt_s[1, h]).T[:, :width].astype(BF16)
        back_copy().start()

    def dv_copy(d):
        k = (i + d) % ns
        return remote(
            dvw_b.at[k], dvw_rx.at[ns - d], dvs.at[d], dvr.at[ns - d], {"sp": k, "tp": t}
        )

    def dv_wait(d):
        k = (i + d) % ns
        return remote(dvw_b.at[k], dvw_rx.at[d], dvs.at[d], dvr.at[d], {"sp": k, "tp": t})

    for k in range(ns):
        dvw_b[k] = dvw_acc[k * lrows : (k + 1) * lrows, :].astype(BF16)
    for d in range(1, ns):
        dv_copy(d).start()

    stage_r2(last)

    @pl.when(last > 3)
    def _():
        stage_r4(last - 3)

    @pl.when(last > 0)
    def _():
        stage_r3(last - 1)

    stage_r3(last)

    def tail(n, carry):
        stage_r4(n)
        return carry

    lax.fori_loop(lax.max(last - 2, 1), lower + 1, tail, 0)

    @pl.when(jnp.logical_not(is_top))
    def _():
        for h in range(heads):
            dq_ref[:, h * width : (h + 1) * width] = (
                (scale * dqt_s[0, h]).T[:, :width].astype(BF16)
            )

    @pl.when(is_top)
    def _():
        back_copy().wait_recv()
        for h in range(heads):
            dq_ref[:, h * width : (h + 1) * width] = (
                (scale * dqt_s[0, h]).T[:, :width]
                + fq_v[:, h * width : (h + 1) * width].astype(F32)
            ).astype(BF16)

    dvw = dvw_acc[pl.ds(pl.multiple_of(i * lrows, lrows), lrows), :]
    for d in range(1, ns):
        dv_wait(d).wait_recv()
        dvw = dvw + dvw_rx[d].astype(F32)
    dvw_ref[...] = dvw

    def add(k, carry):
        o_wait(k).wait_recv()
        own_acc[...] += orx[k].astype(F32)
        return carry

    @pl.when(x == 0)
    def _():
        add(z, 0)

    @pl.when(is_low)
    def _():
        add(nz, 0)

    lax.fori_loop(z + 1, lax.select(is_low, jnp.int32(top), jnp.int32(nz)), add, 0)
    fin[pl.ds(my_piece, piece), :] = own_acc[...].astype(BF16)

    def ag_y(d):
        yy = (y + d) % ny
        return remote(
            fin.at[pl.ds(my_piece, piece)], fin.at[pl.ds(my_piece, piece)], ags.at[d - 1], agr.at[d - 1],
            {"sp": i, "tp": yy * 2 + c},
        )

    def ag_y_wait(d):
        at = pl.multiple_of(c * half + ((y + ny - d) % ny) * piece, piece)
        return remote(
            fin.at[pl.ds(at, piece)], fin.at[pl.ds(at, piece)], ags.at[d - 1], agr.at[d - 1],
            {"sp": i, "tp": ((y + ny - d) % ny) * 2 + c},
        )

    for d in range(1, ny):
        ag_y(d).start()
    for d in range(1, ny):
        ag_y_wait(d).wait_recv()
    ag_c = remote(
        fin.at[pl.ds(my_half, half)], fin.at[pl.ds(my_half, half)], acs.at[0], acr.at[0], core_peer
    )
    ag_c_wait = remote(
        fin.at[pl.ds(peer_half, half)], fin.at[pl.ds(peer_half, half)], acs.at[0], acr.at[0], core_peer
    )
    ag_c.start()

    @pl.when(last > 0)
    def _():
        sends_done(last)

    @pl.when(has_next)
    def _():
        z_copy(i, 0).wait_send()
        z_copy(i, 1).wait_send()

    @pl.when(jnp.logical_or(x == 0, is_low))
    def _():
        x_copy(i, 0).wait_send()
        x_copy(i, 1).wait_send()

    @pl.when(is_top)
    def _():
        for k in range(4):
            visit_copy(k).wait_send()

    @pl.when(is_low)
    def _():
        back_copy().wait_send()

    def drain(n, carry):
        @pl.when(jnp.logical_or(own_column(n), in_plane(n)))
        def _():
            o_copy(n).wait_send()

        @pl.when(for_x_sum(n))
        def _():
            xr_copy(n).wait_send()

        @pl.when(visit_out(n))
        def _():
            v_copy(n).wait_send()

        return carry

    lax.fori_loop(1, last + 1, drain, 0)
    for d in range(1, ns):
        dv_copy(d).wait_send()
    for d in range(1, ny):
        ag_y(d).wait_send()
    ag_c_wait.wait_recv()
    ag_c.wait_send()
    outs = [
        pltpu.make_async_copy(fin.at[:, pl.ds(0, latent_dim)], dlat_hbm, ld.at[0]),
        pltpu.make_async_copy(fin.at[:, pl.ds(latent_dim, WIDE - NOPE)], drope_hbm, ld.at[6]),
    ]
    for out in outs:
        out.start()
    for out in outs:
        out.wait()


def fused_backward(ns, tp, queries, out_grad, attn_out, lse, latent, rope, key_weight, value_weight):
    rows = queries.shape[0]
    latent_dim, hv = key_weight.shape
    heads = hv // NOPE
    packed = latent_dim + rope.shape[1]
    lrows = latent_dim // ns
    ny = tp // 2
    hbm = pl.BlockSpec(memory_space=pl.ANY)
    vmem = pl.BlockSpec(memory_space=pltpu.VMEM)
    dma = pltpu.SemaphoreType.DMA
    return pl.pallas_call(
        functools.partial(fused_kernel, ns, tp, heads, latent_dim),
        in_specs=[hbm, hbm, hbm, vmem, hbm, hbm, hbm, hbm],
        out_specs=[vmem, hbm, hbm, vmem],
        out_shape=[
            jax.ShapeDtypeStruct(queries.shape, BF16),
            jax.ShapeDtypeStruct(latent.shape, BF16),
            jax.ShapeDtypeStruct(rope.shape, BF16),
            jax.ShapeDtypeStruct((lrows, hv), F32),
        ],
        scratch_shapes=[
            pltpu.VMEM(queries.shape, BF16),
            pltpu.VMEM((2,) + out_grad.shape, BF16),
            pltpu.VMEM(queries.shape, BF16),
            pltpu.VMEM((2, heads, rows), F32),
            pltpu.VMEM(attn_out.shape, BF16),
            pltpu.VMEM(key_weight.shape, BF16),
            pltpu.VMEM(value_weight.shape, BF16),
            pltpu.VMEM((2, heads, rows, WIDE), BF16),
            pltpu.VMEM((2, heads, WIDE, rows), BF16),
            pltpu.VMEM((2, heads, VDIM, rows), BF16),
            pltpu.VMEM((2, heads, WIDE, rows), F32),
            pltpu.VMEM((2, heads, rows), F32),
            pltpu.VMEM((heads, rows, WIDE), BF16),
            pltpu.VMEM((heads, WIDE, rows), BF16),
            pltpu.VMEM((rows, hv), BF16),
            pltpu.VMEM((rows, hv), BF16),
            pltpu.VMEM((rows, hv), BF16),
            pltpu.VMEM((latent_dim, hv), F32),
            pltpu.VMEM((ns, lrows, hv), BF16),
            pltpu.VMEM((ns, lrows, hv), BF16),
            pltpu.VMEM((ns + 2, rows, packed), BF16),
            pltpu.VMEM((ns, rows // 2, packed), BF16),
            pltpu.VMEM((ns, max(ny - 1, 1), rows // tp, packed), BF16),
            pltpu.VMEM((ns, rows // tp, packed), BF16),
            pltpu.VMEM((ns // 2 + 1, rows // tp, packed), BF16),
            pltpu.VMEM((rows // tp, packed), F32),
            pltpu.VMEM((rows, packed), BF16),
            dma((7,)),
            dma((ns, 2)),
            dma((ns, 2)),
            dma((ns, 2)),
            dma((ns, 2)),
            dma((ns,)),
            dma((ns,)),
            dma((ns,)),
            dma((ns,)),
            dma((ns,)),
            dma((ns,)),
            dma((ns, max(ny - 1, 1))),
            dma((ns, max(ny - 1, 1))),
            dma((ns // 2 + 1,)),
            dma((ns,)),
            dma((ns,)),
            dma((ns,)),
            dma((max(ny - 1, 1),)),
            dma((max(ny - 1, 1),)),
            dma((1,)),
            dma((1,)),
            dma((5,)),
            dma((5,)),
        ],
        compiler_params=pltpu.CompilerParams(
            collective_id=0, has_side_effects=True, vmem_limit_bytes=67043328
        ),
    )(queries, out_grad, attn_out, lse, latent, rope, key_weight, value_weight)


def per_device(queries, latent, rope_key, key_weight, value_weight, log_sums, attn_out, out_grad):
    rope = jnp.pad(rope_key, ((0, 0), (0, WIDE - NOPE - ROPE)))
    d_queries, dlat, drope, d_value_weight = fused_backward(
        lax.axis_size("sp"), lax.axis_size("tp"),
        queries, out_grad, attn_out, log_sums, latent, rope, key_weight, value_weight,
    )
    d_latent = dlat.astype(F32)
    d_rope = drope[:, :ROPE].astype(F32)
    return (d_queries, d_latent, d_rope, d_value_weight)


def solution(mesh):
    placed = (
        P("sp", "tp"),
        P("sp", None),
        P("sp", None),
        P(None, "tp"),
        P(None, "tp"),
        P("tp", "sp"),
        P("sp", "tp"),
        P("sp", "tp"),
    )
    return jax.shard_map(
        per_device,
        mesh=mesh,
        in_specs=placed,
        out_specs=(P("sp", "tp"), P("sp", None), P("sp", None), P("sp", "tp")),
        check_vma=False,
    )
```

```python
import functools

import jax
import jax.numpy as jnp
from jax import lax
from jax.experimental import pallas as pl
from jax.experimental.pallas import tpu as pltpu
from jax.sharding import PartitionSpec as P

NOPE = 128
ROPE = 64
VDIM = 128
WIDE = 256
LOG2E = 1.4426950408889634
BF16 = jnp.bfloat16
F32 = jnp.float32
MESH = pl.DeviceIdType.MESH


def dot_nn(a, b):
    return lax.dot_general(a, b, (((1,), (0,)), ((), ())), preferred_element_type=F32)


def dot_nt(a, b):
    return lax.dot_general(a, b, (((1,), (1,)), ((), ())), preferred_element_type=F32)


def fused_kernel(
    ns,
    tp,
    heads,
    latent_dim,
    q_hbm,
    g_hbm,
    ao_hbm,
    lse_ref,
    lat_hbm,
    rope_ref,
    wk_hbm,
    wv_hbm,
    dq_ref,
    dlat_hbm,
    drope_ref,
    dvw_ref,
    q_v,
    g_v,
    fq_v,
    lse_s,
    ao_v,
    wk_v,
    wv_v,
    qs_s,
    qt_s,
    gt_s,
    dqt_s,
    delta_s,
    kc_s,
    kct_s,
    v_s,
    dk_s,
    dv_s,
    dvw_acc,
    dvw_b,
    dvx_rx,
    dvw_rx,
    lat_all,
    crx,
    yrx,
    xrx,
    orx,
    own_acc,
    fin,
    ld,
    zr,
    zs,
    xr,
    xs,
    cr,
    cs,
    xrr,
    xrs,
    r1r,
    r1s,
    yr,
    ys,
    orr,
    ors,
    dvr,
    dvs,
    dvxr,
    dvxs,
    agr,
    ags,
    acr,
    acs,
    vr,
    vs,
):
    i = lax.axis_index("sp")
    t = lax.axis_index("tp")
    ny = tp // 2
    nz = ns // 2
    z, x = i // 2, i % 2
    y, c = t // 2, t % 2
    rows, width = q_v.shape[0], NOPE + ROPE
    half, quart, piece = rows // 2, rows // 4, rows // tp
    scale = width ** (-0.5)
    lrows = latent_dim // ns
    chunks = yr.shape[2]
    sub = piece // chunks

    top = nz - 1
    is_top, is_low = z == top, z == 0
    lower = lax.select(is_top, 2 * (z - 1), 2 * z)
    base = lower + x
    last = base + lax.select(is_low, jnp.int32(2), jnp.int32(0))

    def visiting(n):
        return n > base

    def block_of(n):
        down = 2 * (z - 1 - (n - 1) // 2) + (x + n - 1) % 2
        home = lax.select(n == 0, i, lax.select(n > lower, jnp.int32(2 * z), down))
        return lax.select(visiting(n), lax.select(n == base + 1, i, 1 - i), home)

    def key_of(n):
        return lax.select(visiting(n), block_of(n) + 2, block_of(n))

    def part_of(n):
        later = lax.select(is_low, n, block_of(n - 1))
        return lax.select(n == 0, jnp.int32(ns), lax.select(n == 1, jnp.int32(ns + 1), later))

    def own_column(n):
        return jnp.logical_and(n % 2 == 1, n <= lower)

    def for_x_sum(n):
        return jnp.logical_and(jnp.logical_and(n >= 1, n <= lower), n % 2 == 0)

    def in_plane(n):
        return jnp.logical_and(x == 1, n == lower + 1)

    def by_x(n):
        mine = jnp.logical_and(is_low, jnp.logical_and(x == 0, n == base + 2))
        return jnp.logical_or(for_x_sum(n), jnp.logical_or(in_plane(n), mine))

    def visit_out(n):
        return jnp.logical_and(is_low, n == base + 2)

    my_half = pl.multiple_of(c * half, half)
    peer_half = pl.multiple_of((1 - c) * half, half)
    core_peer = {"sp": i, "tp": y * 2 + 1 - c}
    x_peer = {"sp": 2 * z + 1 - x, "tp": t}
    above = {"sp": lax.min(i + 2, ns - 1), "tp": t}

    def remote(src, dst, ssem, rsem, dev):
        return pltpu.make_async_remote_copy(
            src_ref=src, dst_ref=dst, send_sem=ssem, recv_sem=rsem, device_id=dev, device_id_type=MESH
        )

    def lat_rows(j, at, size):
        return lat_all.at[j, pl.ds(at, size)]

    own_cps = [pltpu.make_async_copy(lat_hbm, lat_all.at[i, :, pl.ds(0, latent_dim)], ld.at[0])]
    loads = [
        pltpu.make_async_copy(s, d, ld.at[k + 1])
        for k, (s, d) in enumerate(
            ((g_hbm, g_v.at[0]), (q_hbm, q_v), (ao_hbm, ao_v), (wk_hbm, wk_v), (wv_hbm, wv_v))
        )
    ]
    for cp in own_cps + loads:
        cp.start()

    lat_all[i, :, latent_dim:] = jnp.concatenate(
        [rope_ref[...].T, jnp.zeros((rows, WIDE - NOPE - ROPE), BF16)], axis=1
    )

    barrier = pltpu.get_barrier_semaphore()
    for d in range(1, ns):
        pl.semaphore_signal(
            barrier, inc=1, device_id={"sp": (i + d) % ns, "tp": t}, device_id_type=MESH
        )
    for d in range(1, tp):
        pl.semaphore_signal(
            barrier, inc=1, device_id={"sp": i, "tp": (t + d) % tp}, device_id_type=MESH
        )
    pl.semaphore_wait(barrier, ns - 1 + tp - 1)
    for cp in own_cps:
        cp.wait()

    def quarter(j, k):
        return lat_rows(j, pl.multiple_of(c * half + k * quart, quart), quart)

    def z_copy(j, k):
        return remote(quarter(j, k), quarter(j, k), zs.at[j, k], zr.at[j, k], above)

    def x_copy(j, k):
        return remote(quarter(j, k), quarter(j, k), xs.at[j, k], xr.at[j, k], x_peer)

    def c_copy(j):
        return remote(lat_rows(j, my_half, half), lat_rows(j, my_half, half), cs.at[j], cr.at[j], core_peer)

    has_next = z + 1 < nz

    @pl.when(has_next)
    def _():
        z_copy(i, 0).start()
        z_copy(i, 1).start()

    @pl.when(jnp.logical_or(x == 0, is_low))
    def _():
        x_copy(i, 0).start()

    @pl.when(is_low)
    def _():
        x_copy(i, 1).start()

    def goes_on(n):
        return jnp.logical_and(has_next, jnp.logical_or(z + 1 != top, block_of(n) >= 2))

    low_peer = {"sp": x, "tp": t}
    top_peer = {"sp": 2 * top + x, "tp": t}

    visits = ((g_v.at[0], g_v.at[1]), (q_v, fq_v), (lse_ref, lse_s.at[1]), (delta_s.at[0], delta_s.at[1]))

    def visit_copy(k):
        return remote(visits[k][0], visits[k][1], vs.at[k], vr.at[k], low_peer)

    def back_copy():
        return remote(fq_v, fq_v, vs.at[4], vr.at[4], top_peer)

    def stage_a(n, k):
        @pl.when(own_column(n))
        def _():
            j = block_of(n)
            z_copy(j, k).wait_recv()
            x_copy(j, k).start()

            @pl.when(goes_on(n))
            def _():
                z_copy(j, k).start()

            if k == 1:
                c_copy(j).start()

    def stage_b(n):
        @pl.when(by_x(n))
        def _():
            j = block_of(n)
            x_copy(j, 0).wait_recv()
            x_copy(j, 1).wait_recv()
            c_copy(j).start()

    def sends_done(n):
        j = block_of(n)

        @pl.when(jnp.logical_or(own_column(n), by_x(n)))
        def _():
            c_copy(j).wait_send()

        @pl.when(own_column(n))
        def _():
            for k in range(2):
                x_copy(j, k).wait_send()

            @pl.when(goes_on(n))
            def _():
                for k in range(2):
                    z_copy(j, k).wait_send()

    def r1_copy(n):
        j = key_of(n)
        return remote(
            lat_rows(part_of(n), peer_half, half), crx.at[j], r1s.at[j], r1r.at[j], core_peer
        )

    def rows_of(yy, k):
        return pl.ds(pl.multiple_of(c * half + yy * piece + k * sub, sub), sub)

    def chunk(k):
        return pl.ds(k * sub, sub)

    def y_copy(n, d, k):
        j = key_of(n)
        yy = (y + d) % ny
        return remote(
            lat_all.at[part_of(n), rows_of(yy, k)], yrx.at[j, d - 1, chunk(k)],
            ys.at[j, d - 1, k], yr.at[j, d - 1, k], {"sp": i, "tp": yy * 2 + c},
        )

    def xr_copy(n, k):
        j = block_of(n)
        return remote(
            lat_all.at[part_of(n), rows_of(y, k)], xrx.at[j, chunk(k)], xrs.at[j, k], xrr.at[j, k], x_peer
        )

    def o_copy(n, k):
        return remote(
            lat_all.at[part_of(n), rows_of(y, k)], orx.at[z, chunk(k)], ors.at[key_of(n), k], orr.at[z, k],
            {"sp": block_of(n), "tp": t},
        )

    def v_copy(n, k):
        return remote(
            lat_all.at[part_of(n), rows_of(y, k)], orx.at[nz, chunk(k)], ors.at[key_of(n), k],
            orr.at[nz, k], x_peer,
        )

    def o_wait(zz, k):
        return remote(
            lat_all.at[i, rows_of(y, k)], orx.at[zz, chunk(k)], ors.at[i, k], orr.at[zz, k], x_peer
        )

    def stage_r2(n):
        j = key_of(n)
        b = part_of(n)
        r1_copy(n).wait_recv()

        def add_core(yy, k):
            at = pl.ds(pl.multiple_of(yy * piece + k * sub, sub), sub)
            lat_all[b, rows_of(yy, k), :] = (
                lat_all[b, rows_of(yy, k), :].astype(F32) + crx[j, at, :].astype(F32)
            ).astype(BF16)

        for k in range(chunks):
            for d in range(1, ny):
                add_core((y + d) % ny, k)
                y_copy(n, d, k).start()
        for k in range(chunks):
            add_core(y, k)

    def stage_r3(n):
        j = key_of(n)
        b = part_of(n)
        for k in range(chunks):
            total = lat_all[b, rows_of(y, k), :].astype(F32)
            for d in range(1, ny):
                y_copy(n, d, k).wait_recv()
                total = total + yrx[j, d - 1, k * sub : (k + 1) * sub, :].astype(F32)

            @pl.when(n == 0)
            def _():
                own_acc[k * sub : (k + 1) * sub, :] = total

            @pl.when(jnp.logical_and(is_low, n == base + 1))
            def _():
                own_acc[k * sub : (k + 1) * sub, :] += total

            @pl.when(n > 0)
            def _():
                lat_all[b, rows_of(y, k), :] = total.astype(BF16)

            @pl.when(for_x_sum(n))
            def _():
                xr_copy(n, k).start()

            @pl.when(in_plane(n))
            def _():
                o_copy(n, k).start()

            @pl.when(visit_out(n))
            def _():
                v_copy(n, k).start()

        for k in range(chunks):
            for d in range(1, ny):
                y_copy(n, d, k).wait_send()
        r1_copy(n).wait_send()

    def stage_r4(n):
        @pl.when(own_column(n))
        def _():
            j = block_of(n)
            b = part_of(n)
            for k in range(chunks):
                xr_copy(n, k).wait_recv()
                total = (
                    lat_all[b, rows_of(y, k), :].astype(F32)
                    + xrx[j, k * sub : (k + 1) * sub, :].astype(F32)
                )
                lat_all[b, rows_of(y, k), :] = total.astype(BF16)
                o_copy(n, k).start()

    def prepare(qi, q_ref):
        for h in range(heads):
            qh = jnp.concatenate(
                [q_ref[:, h * width : (h + 1) * width], jnp.zeros((rows, WIDE - width), BF16)], axis=1
            )
            qs_s[qi, h] = qh
            qt_s[qi, h] = qh.T
            gt_s[qi, h] = g_v[qi, :, h * VDIM : (h + 1) * VDIM].T
        dqt_s[qi] = jnp.zeros_like(dqt_s[qi])

    for cp in loads[:2]:
        cp.wait()

    @pl.when(is_top)
    def _():
        for k in range(3):
            visit_copy(k).start()

    for cp in loads[2:]:
        cp.wait()
    prepare(0, q_v)
    for h in range(heads):
        at = ao_v[:, h * VDIM : (h + 1) * VDIM].T
        delta_s[0, h : h + 1, :] = jnp.sum(
            gt_s[0, h].astype(F32) * at.astype(F32), axis=0, keepdims=True
        )
    lse_s[0] = lse_ref[...]

    @pl.when(is_top)
    def _():
        visit_copy(3).start()

    dvw_acc[...] = jnp.zeros_like(dvw_acc)

    def slot(n, carry):
        j = block_of(n)
        b = part_of(n)
        qi = lax.select(visiting(n), jnp.int32(1), jnp.int32(0))
        q_block = lax.select(visiting(n), 2 * top + x, i)

        @pl.when(jnp.logical_or(own_column(n), by_x(n)))
        def _():
            c_copy(j).wait_recv()

        @pl.when(n == base + 1)
        def _():
            for k in range(4):
                visit_copy(k).wait_recv()
            prepare(1, fq_v)

        rope = lat_all[j, :, latent_dim:]
        keys = dot_nn(lat_all[j, :, :latent_dim], wk_v[...]).astype(BF16)
        v_s[...] = dot_nn(lat_all[j, :, :latent_dim], wv_v[...]).astype(BF16)
        for h in range(heads):
            kc = jnp.concatenate([keys[:, h * NOPE : (h + 1) * NOPE], rope], axis=1)
            kc_s[h] = kc
            kct_s[h] = kc.T
        rope_sum = jnp.zeros((rows, WIDE - NOPE), F32)
        k_pos = lax.broadcasted_iota(jnp.int32, (rows, rows), 0)
        q_pos = lax.broadcasted_iota(jnp.int32, (rows, rows), 1)
        causal = k_pos - q_pos <= (q_block - j) * rows
        for h in range(heads):
            s = dot_nn(kc_s[h], qt_s[qi, h])
            zz = s * (scale * LOG2E) - lse_s[qi, h : h + 1, :] * LOG2E
            p = jnp.exp2(jnp.where(causal, zz, -1e30))
            dp = dot_nn(v_s[:, h * VDIM : (h + 1) * VDIM], gt_s[qi, h])
            ds = (p * (dp - delta_s[qi, h : h + 1, :])).astype(BF16)
            dv_s[:, h * VDIM : (h + 1) * VDIM] = dot_nn(
                p.astype(BF16), g_v[qi, :, h * VDIM : (h + 1) * VDIM]
            ).astype(BF16)
            dk = scale * dot_nn(ds, qs_s[qi, h])
            dk_s[:, h * NOPE : (h + 1) * NOPE] = dk[:, :NOPE].astype(BF16)
            rope_sum = rope_sum + dk[:, NOPE:]
            dqt_s[qi, h] += dot_nn(kct_s[h], ds)
            if h == 0:

                @pl.when(n > 0)
                def _():
                    stage_r2(n - 1)

            if h == (heads - 1) // 2:

                @pl.when(n > 1)
                def _():
                    stage_a(n + 1, 1)
                    stage_r3(n - 2)

            if h == heads // 2:

                @pl.when(n == 0)
                def _():
                    stage_a(n + 1, 0)

        @pl.when(n > 4)
        def _():
            stage_r4(n - 4)

        @pl.when(n > 1)
        def _():
            sends_done(n - 1)

        dlat = dot_nt(dk_s[...], wk_v[...]) + dot_nt(dv_s[...], wv_v[...])
        lat_all[b, :, :latent_dim] = dlat.astype(BF16)
        lat_all[b, :, latent_dim:] = rope_sum.astype(BF16)
        r1_copy(n).start()

        @pl.when(n == 0)
        def _():
            stage_a(n + 1, 1)

        stage_b(n + 1)
        dvw_acc[...] += dot_nn(lat_all[j, :, :latent_dim].T, dv_s[...])

        @pl.when(n > 0)
        def _():
            stage_a(n + 2, 0)

        @pl.when(jnp.logical_and(jnp.logical_and(x == 0, z > 0), n == 2))
        def _():
            x_copy(i, 1).start()

        return carry

    lax.fori_loop(0, last + 1, slot, 0)

    @pl.when(is_low)
    def _():
        for h in range(heads):
            fq_v[:, h * width : (h + 1) * width] = (scale * dqt_s[1, h]).T[:, :width].astype(BF16)
        back_copy().start()

    def wrows(k):
        return pl.ds(pl.multiple_of(k * lrows, lrows), lrows)

    def dvx_copy():
        return remote(dvw_b.at[1 - x], dvx_rx, dvxs.at[0], dvxr.at[0], x_peer)

    def dv_copy(d):
        zz = (z + d) % nz
        return remote(
            dvw_b.at[x, zz], dvw_rx.at[nz - d], dvs.at[d], dvr.at[nz - d], {"sp": 2 * zz + x, "tp": t}
        )

    def dv_wait(d):
        return remote(dvw_b.at[x, z], dvw_rx.at[d], dvs.at[d], dvr.at[d], x_peer)

    for k in range(ns):
        dvw_b[k % 2, k // 2] = dvw_acc[k * lrows : (k + 1) * lrows, :].astype(BF16)

    @pl.when(x == 0)
    def _():
        dvx_copy().start()

    stage_r2(last)

    @pl.when(last > 3)
    def _():
        stage_r4(last - 3)

    @pl.when(last > 0)
    def _():
        stage_r3(last - 1)

    @pl.when(x == 1)
    def _():
        dvx_copy().start()

    @pl.when(jnp.logical_not(is_top))
    def _():
        for h in range(heads):
            dq_ref[:, h * width : (h + 1) * width] = (
                (scale * dqt_s[0, h]).T[:, :width].astype(BF16)
            )

    stage_r3(last)

    def tail(n, carry):
        stage_r4(n)
        return carry

    lax.fori_loop(lax.max(last - 2, 1), lower + 1, tail, 0)
    dvx_copy().wait_recv()
    dvx_copy().wait_send()
    for d in range(1, nz):
        zz = (z + d) % nz
        dvw_b[x, zz] = (dvw_acc[wrows(2 * zz + x), :] + dvx_rx[zz].astype(F32)).astype(BF16)
        dv_copy(d).start()

    @pl.when(is_top)
    def _():
        back_copy().wait_recv()
        for h in range(heads):
            dq_ref[:, h * width : (h + 1) * width] = (
                (scale * dqt_s[0, h]).T[:, :width]
                + fq_v[:, h * width : (h + 1) * width].astype(F32)
            ).astype(BF16)

    def ag_y(d, k):
        yy = (y + d) % ny
        return remote(
            fin.at[rows_of(y, k)], fin.at[rows_of(y, k)], ags.at[d - 1, k], agr.at[d - 1, k],
            {"sp": i, "tp": yy * 2 + c},
        )

    def ag_y_wait(d, k):
        yy = (y + ny - d) % ny
        return remote(
            fin.at[rows_of(yy, k)], fin.at[rows_of(yy, k)], ags.at[d - 1, k], agr.at[d - 1, k],
            {"sp": i, "tp": yy * 2 + c},
        )

    for k in range(chunks):

        def add(zz, carry):
            o_wait(zz, k).wait_recv()
            own_acc[k * sub : (k + 1) * sub, :] += orx[zz, k * sub : (k + 1) * sub, :].astype(F32)
            return carry

        @pl.when(x == 0)
        def _():
            add(z, 0)

        @pl.when(is_low)
        def _():
            add(nz, 0)

        lax.fori_loop(z + 1, lax.select(is_low, jnp.int32(top), jnp.int32(nz)), add, 0)
        fin[rows_of(y, k), :] = own_acc[k * sub : (k + 1) * sub, :].astype(BF16)
        for d in range(1, ny):
            ag_y(d, k).start()

    dvw = dvw_acc[wrows(i), :] + dvx_rx[z].astype(F32)
    for d in range(1, nz):
        dv_wait(d).wait_recv()
        dvw = dvw + dvw_rx[d].astype(F32)
    dvw_ref[...] = dvw
    for k in range(chunks):
        for d in range(1, ny):
            ag_y_wait(d, k).wait_recv()
    ag_c = remote(
        fin.at[pl.ds(my_half, half)], fin.at[pl.ds(my_half, half)], acs.at[0], acr.at[0], core_peer
    )
    ag_c_wait = remote(
        fin.at[pl.ds(peer_half, half)], fin.at[pl.ds(peer_half, half)], acs.at[0], acr.at[0], core_peer
    )
    ag_c.start()

    def out_copy(at, k):
        return pltpu.make_async_copy(
            fin.at[pl.ds(at, half), pl.ds(0, latent_dim)], dlat_hbm.at[pl.ds(at, half)], ld.at[k]
        )

    out_copy(my_half, 0).start()

    @pl.when(last > 0)
    def _():
        sends_done(last)

    @pl.when(has_next)
    def _():
        z_copy(i, 0).wait_send()
        z_copy(i, 1).wait_send()

    @pl.when(jnp.logical_or(x == 0, is_low))
    def _():
        x_copy(i, 0).wait_send()
        x_copy(i, 1).wait_send()

    @pl.when(is_top)
    def _():
        for k in range(4):
            visit_copy(k).wait_send()

    @pl.when(is_low)
    def _():
        back_copy().wait_send()

    def drain(n, carry):
        @pl.when(jnp.logical_or(own_column(n), in_plane(n)))
        def _():
            for k in range(chunks):
                o_copy(n, k).wait_send()

        @pl.when(for_x_sum(n))
        def _():
            for k in range(chunks):
                xr_copy(n, k).wait_send()

        @pl.when(visit_out(n))
        def _():
            for k in range(chunks):
                v_copy(n, k).wait_send()

        return carry

    lax.fori_loop(1, last + 1, drain, 0)
    for d in range(1, nz):
        dv_copy(d).wait_send()
    for k in range(chunks):
        for d in range(1, ny):
            ag_y(d, k).wait_send()
    ag_c_wait.wait_recv()
    ag_c.wait_send()
    out_copy(peer_half, 1).start()
    drope_ref[...] = fin[:, latent_dim : latent_dim + ROPE].astype(F32).T
    out_copy(my_half, 0).wait()
    out_copy(peer_half, 1).wait()


def fused_backward(ns, tp, queries, out_grad, attn_out, lse, latent, rope_t, key_weight, value_weight):
    rows = queries.shape[0]
    latent_dim, hv = key_weight.shape
    heads = hv // NOPE
    packed = latent_dim + WIDE - NOPE
    lrows = latent_dim // ns
    ny = tp // 2
    chunks = min(4, rows // tp // 32)
    hbm = pl.BlockSpec(memory_space=pl.ANY)
    vmem = pl.BlockSpec(memory_space=pltpu.VMEM)
    dma = pltpu.SemaphoreType.DMA
    return pl.pallas_call(
        functools.partial(fused_kernel, ns, tp, heads, latent_dim),
        in_specs=[hbm, hbm, hbm, vmem, hbm, vmem, hbm, hbm],
        out_specs=[vmem, hbm, vmem, vmem],
        out_shape=[
            jax.ShapeDtypeStruct(queries.shape, BF16),
            jax.ShapeDtypeStruct(latent.shape, BF16),
            jax.ShapeDtypeStruct(rope_t.shape, F32),
            jax.ShapeDtypeStruct((lrows, hv), F32),
        ],
        scratch_shapes=[
            pltpu.VMEM(queries.shape, BF16),
            pltpu.VMEM((2,) + out_grad.shape, BF16),
            pltpu.VMEM(queries.shape, BF16),
            pltpu.VMEM((2, heads, rows), F32),
            pltpu.VMEM(attn_out.shape, BF16),
            pltpu.VMEM(key_weight.shape, BF16),
            pltpu.VMEM(value_weight.shape, BF16),
            pltpu.VMEM((2, heads, rows, WIDE), BF16),
            pltpu.VMEM((2, heads, WIDE, rows), BF16),
            pltpu.VMEM((2, heads, VDIM, rows), BF16),
            pltpu.VMEM((2, heads, WIDE, rows), F32),
            pltpu.VMEM((2, heads, rows), F32),
            pltpu.VMEM((heads, rows, WIDE), BF16),
            pltpu.VMEM((heads, WIDE, rows), BF16),
            pltpu.VMEM((rows, hv), BF16),
            pltpu.VMEM((rows, hv), BF16),
            pltpu.VMEM((rows, hv), BF16),
            pltpu.VMEM((latent_dim, hv), F32),
            pltpu.VMEM((2, ns // 2, lrows, hv), BF16),
            pltpu.VMEM((ns // 2, lrows, hv), BF16),
            pltpu.VMEM((ns // 2, lrows, hv), BF16),
            pltpu.VMEM((ns + 2, rows, packed), BF16),
            pltpu.VMEM((ns, rows // 2, packed), BF16),
            pltpu.VMEM((ns, max(ny - 1, 1), rows // tp, packed), BF16),
            pltpu.VMEM((ns, rows // tp, packed), BF16),
            pltpu.VMEM((ns // 2 + 1, rows // tp, packed), BF16),
            pltpu.VMEM((rows // tp, packed), F32),
            pltpu.VMEM((rows, packed), BF16),
            dma((6,)),
            dma((ns, 2)),
            dma((ns, 2)),
            dma((ns, 2)),
            dma((ns, 2)),
            dma((ns,)),
            dma((ns,)),
            dma((ns, chunks)),
            dma((ns, chunks)),
            dma((ns,)),
            dma((ns,)),
            dma((ns, max(ny - 1, 1), chunks)),
            dma((ns, max(ny - 1, 1), chunks)),
            dma((ns // 2 + 1, chunks)),
            dma((ns, chunks)),
            dma((ns // 2,)),
            dma((ns // 2,)),
            dma((1,)),
            dma((1,)),
            dma((max(ny - 1, 1), chunks)),
            dma((max(ny - 1, 1), chunks)),
            dma((1,)),
            dma((1,)),
            dma((5,)),
            dma((5,)),
        ],
        compiler_params=pltpu.CompilerParams(
            collective_id=0, has_side_effects=True, vmem_limit_bytes=67043328
        ),
    )(queries, out_grad, attn_out, lse, latent, rope_t, key_weight, value_weight)


def per_device(queries, latent, rope_key, key_weight, value_weight, log_sums, attn_out, out_grad):
    d_queries, dlat, drope_t, d_value_weight = fused_backward(
        lax.axis_size("sp"), lax.axis_size("tp"),
        queries, out_grad, attn_out, log_sums, latent, rope_key.T, key_weight, value_weight,
    )
    d_latent = dlat.astype(F32)
    d_rope = drope_t.T
    return (d_queries, d_latent, d_rope, d_value_weight)


def solution(mesh):
    placed = (
        P("sp", "tp"),
        P("sp", None),
        P("sp", None),
        P(None, "tp"),
        P(None, "tp"),
        P("tp", "sp"),
        P("sp", "tp"),
        P("sp", "tp"),
    )
    return jax.shard_map(
        per_device,
        mesh=mesh,
        in_specs=placed,
        out_specs=(P("sp", "tp"), P("sp", None), P("sp", None), P("sp", "tp")),
        check_vma=False,
    )
```

```python
import functools

import jax
import jax.numpy as jnp
from jax import lax
from jax.experimental import pallas as pl
from jax.experimental.pallas import tpu as pltpu
from jax.sharding import PartitionSpec as P

NOPE = 128
ROPE = 64
VDIM = 128
WIDE = 256
LOG2E = 1.4426950408889634
BF16 = jnp.bfloat16
F32 = jnp.float32
MESH = pl.DeviceIdType.MESH


def dot_nn(a, b):
    return lax.dot_general(a, b, (((1,), (0,)), ((), ())), preferred_element_type=F32)


def dot_nt(a, b):
    return lax.dot_general(a, b, (((1,), (1,)), ((), ())), preferred_element_type=F32)


def fused_kernel(
    ns,
    tp,
    heads,
    latent_dim,
    q_hbm,
    g_hbm,
    ao_hbm,
    lse_ref,
    lat_hbm,
    rope_ref,
    wk_hbm,
    wv_hbm,
    dq_hbm,
    dlat_hbm,
    drope_ref,
    dvw_ref,
    q_v,
    g_v,
    fq_v,
    lse_s,
    ao_v,
    wk_v,
    wv_v,
    qs_s,
    qt_s,
    gt_s,
    dqt_s,
    delta_s,
    kc_s,
    kct_s,
    lat_t,
    v_s,
    dk_s,
    dv_s,
    dvw_acc,
    dvw_b,
    dvx_rx,
    dvw_rx,
    lat_all,
    crx,
    yrx,
    xrx,
    orx,
    own_acc,
    fin,
    ld,
    zr,
    zs,
    xr,
    xs,
    cr,
    cs,
    xrr,
    xrs,
    r1r,
    r1s,
    yr,
    ys,
    orr,
    ors,
    dvr,
    dvs,
    dvxr,
    dvxs,
    agr,
    ags,
    acr,
    acs,
    vr,
    vs,
):
    i = lax.axis_index("sp")
    t = lax.axis_index("tp")
    ny = tp // 2
    nz = ns // 2
    z, x = i // 2, i % 2
    y, c = t // 2, t % 2
    rows, width = q_v.shape[0], NOPE + ROPE
    half, piece = rows // 2, rows // tp
    parts = zr.shape[1]
    bit = half // parts
    early, late = range(parts // 2), range(parts // 2, parts)
    scale = width ** (-0.5)
    lrows = latent_dim // ns
    chunks = yr.shape[2]
    sub = piece // chunks

    top = nz - 1
    is_top, is_low = z == top, z == 0
    lower = lax.select(is_top, 2 * (z - 1), 2 * z)
    base = lower + x
    last = base + lax.select(is_low, jnp.int32(2), jnp.int32(0))

    def visiting(n):
        return n > base

    def block_of(n):
        down = 2 * (z - 1 - (n - 1) // 2) + (x + n - 1) % 2
        home = lax.select(n == 0, i, lax.select(n > lower, jnp.int32(2 * z), down))
        return lax.select(visiting(n), lax.select(n == base + 1, i, 1 - i), home)

    def key_of(n):
        return lax.select(visiting(n), block_of(n) + 2, block_of(n))

    def part_of(n):
        later = lax.select(is_low, n, block_of(n - 1))
        return lax.select(n == 0, jnp.int32(ns), lax.select(n == 1, jnp.int32(ns + 1), later))

    def own_column(n):
        return jnp.logical_and(n % 2 == 1, n <= lower)

    def for_x_sum(n):
        return jnp.logical_and(jnp.logical_and(n >= 1, n <= lower), n % 2 == 0)

    def in_plane(n):
        return jnp.logical_and(x == 1, n == lower + 1)

    def by_x(n):
        mine = jnp.logical_and(is_low, jnp.logical_and(x == 0, n == base + 2))
        return jnp.logical_or(for_x_sum(n), jnp.logical_or(in_plane(n), mine))

    def visit_out(n):
        return jnp.logical_and(is_low, n == base + 2)

    my_half = pl.multiple_of(c * half, half)
    peer_half = pl.multiple_of((1 - c) * half, half)
    core_peer = {"sp": i, "tp": y * 2 + 1 - c}
    x_peer = {"sp": 2 * z + 1 - x, "tp": t}
    above = {"sp": lax.min(i + 2, ns - 1), "tp": t}

    def remote(src, dst, ssem, rsem, dev):
        return pltpu.make_async_remote_copy(
            src_ref=src, dst_ref=dst, send_sem=ssem, recv_sem=rsem, device_id=dev, device_id_type=MESH
        )

    def lat_rows(j, at, size):
        return lat_all.at[j, pl.ds(at, size)]

    own_cps = [pltpu.make_async_copy(lat_hbm, lat_all.at[i, :, pl.ds(0, latent_dim)], ld.at[0])]
    loads = [
        pltpu.make_async_copy(s, d, ld.at[k + 1])
        for k, (s, d) in enumerate(
            ((g_hbm, g_v.at[0]), (q_hbm, q_v), (ao_hbm, ao_v), (wk_hbm, wk_v), (wv_hbm, wv_v))
        )
    ]
    for cp in own_cps + loads:
        cp.start()

    lat_all[i, :, latent_dim:] = jnp.concatenate(
        [rope_ref[...].T, jnp.zeros((rows, WIDE - NOPE - ROPE), BF16)], axis=1
    )

    barrier = pltpu.get_barrier_semaphore()
    for d in range(1, ns):
        pl.semaphore_signal(
            barrier, inc=1, device_id={"sp": (i + d) % ns, "tp": t}, device_id_type=MESH
        )
    for d in range(1, tp):
        pl.semaphore_signal(
            barrier, inc=1, device_id={"sp": i, "tp": (t + d) % tp}, device_id_type=MESH
        )
    pl.semaphore_wait(barrier, ns - 1 + tp - 1)
    for cp in own_cps:
        cp.wait()

    def bit_of(j, k):
        return lat_rows(j, pl.multiple_of(c * half + k * bit, bit), bit)

    def z_copy(j, k):
        return remote(bit_of(j, k), bit_of(j, k), zs.at[j, k], zr.at[j, k], above)

    def x_copy(j, k):
        return remote(bit_of(j, k), bit_of(j, k), xs.at[j, k], xr.at[j, k], x_peer)

    def c_copy(j, k):
        return remote(bit_of(j, k), bit_of(j, k), cs.at[j, k], cr.at[j, k], core_peer)

    has_next = z + 1 < nz

    @pl.when(has_next)
    def _():
        for k in range(parts):
            z_copy(i, k).start()

    @pl.when(jnp.logical_or(x == 0, is_low))
    def _():
        for k in early:
            x_copy(i, k).start()

    @pl.when(is_low)
    def _():
        for k in late:
            x_copy(i, k).start()

    def goes_on(n):
        return jnp.logical_and(has_next, jnp.logical_or(z + 1 != top, block_of(n) >= 2))

    low_peer = {"sp": x, "tp": t}
    top_peer = {"sp": 2 * top + x, "tp": t}

    visits = ((g_v.at[0], g_v.at[1]), (q_v, fq_v), (lse_ref, lse_s.at[1]), (delta_s.at[0], delta_s.at[1]))

    def visit_copy(k):
        return remote(visits[k][0], visits[k][1], vs.at[k], vr.at[k], low_peer)

    def back_copy():
        return remote(fq_v, fq_v, vs.at[4], vr.at[4], top_peer)

    def stage_a(n, pieces):
        @pl.when(own_column(n))
        def _():
            j = block_of(n)
            for k in pieces:
                z_copy(j, k).wait_recv()
                x_copy(j, k).start()
                c_copy(j, k).start()

                @pl.when(goes_on(n))
                def _():
                    z_copy(j, k).start()

    def stage_b(n):
        j = block_of(n)
        for k in range(parts):
            x_copy(j, k).wait_recv()
            c_copy(j, k).start()

    def sends_done(n):
        j = block_of(n)

        @pl.when(jnp.logical_or(own_column(n), by_x(n)))
        def _():
            for k in range(parts):
                c_copy(j, k).wait_send()

        @pl.when(own_column(n))
        def _():
            for k in range(parts):
                x_copy(j, k).wait_send()

            @pl.when(goes_on(n))
            def _():
                for k in range(parts):
                    z_copy(j, k).wait_send()

    def r1_copy(n):
        j = key_of(n)
        return remote(
            lat_rows(part_of(n), peer_half, half), crx.at[j], r1s.at[j], r1r.at[j], core_peer
        )

    def rows_of(yy, k):
        return pl.ds(pl.multiple_of(c * half + yy * piece + k * sub, sub), sub)

    def chunk(k):
        return pl.ds(k * sub, sub)

    def y_copy(n, d, k):
        j = key_of(n)
        yy = (y + d) % ny
        return remote(
            lat_all.at[part_of(n), rows_of(yy, k)], yrx.at[j, d - 1, chunk(k)],
            ys.at[j, d - 1, k], yr.at[j, d - 1, k], {"sp": i, "tp": yy * 2 + c},
        )

    def xr_copy(n, k):
        j = block_of(n)
        return remote(
            lat_all.at[part_of(n), rows_of(y, k)], xrx.at[j, chunk(k)], xrs.at[j, k], xrr.at[j, k], x_peer
        )

    def o_copy(n, k):
        return remote(
            lat_all.at[part_of(n), rows_of(y, k)], orx.at[z, chunk(k)], ors.at[key_of(n), k], orr.at[z, k],
            {"sp": block_of(n), "tp": t},
        )

    def v_copy(n, k):
        return remote(
            lat_all.at[part_of(n), rows_of(y, k)], orx.at[nz, chunk(k)], ors.at[key_of(n), k],
            orr.at[nz, k], x_peer,
        )

    def o_wait(zz, k):
        return remote(
            lat_all.at[i, rows_of(y, k)], orx.at[zz, chunk(k)], ors.at[i, k], orr.at[zz, k], x_peer
        )

    def stage_r2(n):
        j = key_of(n)
        b = part_of(n)
        r1_copy(n).wait_recv()

        def add_core(yy, k):
            at = pl.ds(pl.multiple_of(yy * piece + k * sub, sub), sub)
            lat_all[b, rows_of(yy, k), :] = lat_all[b, rows_of(yy, k), :] + crx[j, at, :]

        for k in range(chunks):
            for d in range(1, ny):
                add_core((y + d) % ny, k)
                y_copy(n, d, k).start()
        for k in range(chunks):
            add_core(y, k)

    def stage_r3(n):
        j = key_of(n)
        b = part_of(n)
        for k in range(chunks):
            total = lat_all[b, rows_of(y, k), :].astype(F32)
            for d in range(1, ny):
                y_copy(n, d, k).wait_recv()
                total = total + yrx[j, d - 1, k * sub : (k + 1) * sub, :].astype(F32)

            @pl.when(n == 0)
            def _():
                own_acc[k * sub : (k + 1) * sub, :] = total

            @pl.when(jnp.logical_and(is_low, n == base + 1))
            def _():
                own_acc[k * sub : (k + 1) * sub, :] += total

            @pl.when(n > 0)
            def _():
                lat_all[b, rows_of(y, k), :] = total.astype(BF16)

            @pl.when(for_x_sum(n))
            def _():
                xr_copy(n, k).start()

            @pl.when(in_plane(n))
            def _():
                o_copy(n, k).start()

            @pl.when(visit_out(n))
            def _():
                v_copy(n, k).start()

        for k in range(chunks):
            for d in range(1, ny):
                y_copy(n, d, k).wait_send()
        r1_copy(n).wait_send()

    def stage_r4(n):
        @pl.when(own_column(n))
        def _():
            j = block_of(n)
            b = part_of(n)
            for k in range(chunks):
                xr_copy(n, k).wait_recv()
                total = (
                    lat_all[b, rows_of(y, k), :].astype(F32)
                    + xrx[j, k * sub : (k + 1) * sub, :].astype(F32)
                )
                lat_all[b, rows_of(y, k), :] = total.astype(BF16)
                o_copy(n, k).start()

    def prepare(qi, q_ref):
        for h in range(heads):
            qh = jnp.concatenate(
                [q_ref[:, h * width : (h + 1) * width], jnp.zeros((rows, WIDE - width), BF16)], axis=1
            )
            qs_s[qi, h] = qh
            qt_s[qi, h] = qh.T
            gt_s[qi, h] = g_v[qi, :, h * VDIM : (h + 1) * VDIM].T
        dqt_s[qi] = jnp.zeros_like(dqt_s[qi])

    for cp in loads[:2]:
        cp.wait()

    @pl.when(is_top)
    def _():
        for k in range(3):
            visit_copy(k).start()

    for cp in loads[2:]:
        cp.wait()
    prepare(0, q_v)
    for h in range(heads):
        at = ao_v[:, h * VDIM : (h + 1) * VDIM].T
        delta_s[0, h : h + 1, :] = jnp.sum(
            gt_s[0, h].astype(F32) * at.astype(F32), axis=0, keepdims=True
        )
    lse_s[0] = lse_ref[...]

    @pl.when(is_top)
    def _():
        visit_copy(3).start()

    dvw_acc[...] = jnp.zeros_like(dvw_acc)

    def slot(n, diagonal):
        j = block_of(n)
        b = part_of(n)
        qi = lax.select(visiting(n), jnp.int32(1), jnp.int32(0))

        if not diagonal:

            @pl.when(jnp.logical_or(own_column(n), by_x(n)))
            def _():
                for k in range(parts):
                    c_copy(j, k).wait_recv()

            @pl.when(n == base + 1)
            def _():
                for k in range(4):
                    visit_copy(k).wait_recv()
                prepare(1, fq_v)

        rope = lat_all[j, :, latent_dim:]
        rope_t = rope.T[:ROPE]
        lat_t[...] = lat_all[j, :, :latent_dim].T
        keys = dot_nn(lat_all[j, :, :latent_dim], wk_v[...]).astype(BF16)
        v_s[...] = dot_nn(lat_all[j, :, :latent_dim], wv_v[...]).astype(BF16)
        for h in range(heads):
            kc = jnp.concatenate([keys[:, h * NOPE : (h + 1) * NOPE], rope], axis=1)
            kc_s[h] = kc
            kct_s[h, :NOPE] = keys[:, h * NOPE : (h + 1) * NOPE].T
            kct_s[h, NOPE:] = rope_t
        rope_sum = jnp.zeros((rows, WIDE - NOPE), F32)
        for h in range(heads):
            s = dot_nn(kc_s[h], qt_s[qi, h])
            zz = s * (scale * LOG2E) - lse_s[qi, h : h + 1, :] * LOG2E
            if diagonal:
                k_pos = lax.broadcasted_iota(jnp.int32, (rows, rows), 0)
                q_pos = lax.broadcasted_iota(jnp.int32, (rows, rows), 1)
                zz = jnp.where(k_pos <= q_pos, zz, -1e30)
            p = jnp.exp2(zz)
            dp = dot_nn(v_s[:, h * VDIM : (h + 1) * VDIM], gt_s[qi, h])
            ds = (p * (dp - delta_s[qi, h : h + 1, :])).astype(BF16)
            dv_s[:, h * VDIM : (h + 1) * VDIM] = dot_nn(
                p.astype(BF16), g_v[qi, :, h * VDIM : (h + 1) * VDIM]
            ).astype(BF16)
            dk = scale * dot_nn(ds, qs_s[qi, h])
            dk_s[:, h * NOPE : (h + 1) * NOPE] = dk[:, :NOPE].astype(BF16)
            rope_sum = rope_sum + dk[:, NOPE:]
            dqt_s[qi, h] += dot_nn(kct_s[h], ds)
            if h == heads // 2 - 1 and not diagonal:
                stage_r2(n - 1)

                @pl.when(n > 1)
                def _():
                    stage_a(n + 1, late)

        if not diagonal:

            @pl.when(n > 1)
            def _():
                stage_r3(n - 2)
                sends_done(n - 1)

                @pl.when(n > 4)
                def _():
                    stage_r4(n - 4)

                @pl.when(in_plane(n + 1))
                def _():
                    stage_b(n + 1)

        dlat = dot_nt(dk_s[...], wk_v[...]) + dot_nt(dv_s[...], wv_v[...])
        lat_all[b, :, :latent_dim] = dlat.astype(BF16)
        lat_all[b, :, latent_dim:] = rope_sum.astype(BF16)
        r1_copy(n).start()

        if diagonal:
            stage_a(n + 1, range(parts))

        @pl.when(jnp.logical_and(by_x(n + 1), jnp.logical_or(is_low, jnp.logical_not(in_plane(n + 1)))))
        def _():
            stage_b(n + 1)

        dvw_acc[...] += dot_nn(lat_t[...], dv_s[...])

        if not diagonal:
            stage_a(n + 2, early)

            @pl.when(jnp.logical_and(jnp.logical_and(x == 0, z > 0), n == 2))
            def _():
                for k in late:
                    x_copy(i, k).start()

    slot(jnp.int32(0), True)

    def later_slot(n, carry):
        slot(n, False)
        return carry

    lax.fori_loop(1, last + 1, later_slot, 0)

    @pl.when(is_low)
    def _():
        for h in range(heads):
            fq_v[:, h * width : (h + 1) * width] = (scale * dqt_s[1, h]).T.astype(BF16)
        back_copy().start()

    def wrows(k):
        return pl.ds(pl.multiple_of(k * lrows, lrows), lrows)

    def dvx_copy(d):
        zz = (z + d) % nz
        return remote(dvw_b.at[1 - x, zz], dvx_rx.at[zz], dvxs.at[d], dvxr.at[d], x_peer)

    send_order = tuple(range(1, nz)) + (0,)

    def dv_copy(d):
        zz = (z + d) % nz
        return remote(
            dvw_b.at[x, zz], dvw_rx.at[nz - d], dvs.at[d], dvr.at[nz - d], {"sp": 2 * zz + x, "tp": t}
        )

    def dv_wait(d):
        return remote(dvw_b.at[x, z], dvw_rx.at[d], dvs.at[d], dvr.at[d], x_peer)

    for k in range(ns):
        dvw_b[k % 2, k // 2] = dvw_acc[k * lrows : (k + 1) * lrows, :].astype(BF16)

    stage_r2(last)

    @pl.when(last > 3)
    def _():
        stage_r4(last - 3)

    @pl.when(last > 0)
    def _():
        stage_r3(last - 1)

    @pl.when(x == 1)
    def _():
        for d in send_order:
            dvx_copy(d).start()

        @pl.when(last > 2)
        def _():
            stage_r4(last - 2)

    @pl.when(jnp.logical_not(is_top))
    def _():
        for h in range(heads):
            q_v[:, h * width : (h + 1) * width] = (
                (scale * dqt_s[0, h]).T.astype(BF16)
            )

    stage_r3(last)

    @pl.when(x == 0)
    def _():
        for d in send_order:
            dvx_copy(d).start()

    def tail(n, carry):
        stage_r4(n)
        return carry

    lax.fori_loop(lax.max(last - 2 + x, 1), lower + 1, tail, 0)
    for d in range(1, nz):
        dvx_copy(d).wait_recv()
        zz = (z + d) % nz
        dvw_b[x, zz] = (dvw_acc[wrows(2 * zz + x), :] + dvx_rx[zz].astype(F32)).astype(BF16)
        dv_copy(d).start()

    @pl.when(is_top)
    def _():
        for k in range(4):
            visit_copy(k).wait_send()
        back_copy().wait_recv()
        for h in range(heads):
            q_v[:, h * width : (h + 1) * width] = (
                (scale * dqt_s[0, h]).T
                + fq_v[:, h * width : (h + 1) * width].astype(F32)
            ).astype(BF16)

    dq_out = pltpu.make_async_copy(q_v, dq_hbm, ld.at[2])
    dq_out.start()

    def ag_y(d, k):
        yy = (y + d) % ny
        return remote(
            fin.at[rows_of(y, k)], fin.at[rows_of(y, k)], ags.at[d - 1, k], agr.at[d - 1, k],
            {"sp": i, "tp": yy * 2 + c},
        )

    def ag_y_wait(d, k):
        yy = (y + ny - d) % ny
        return remote(
            fin.at[rows_of(yy, k)], fin.at[rows_of(yy, k)], ags.at[d - 1, k], agr.at[d - 1, k],
            {"sp": i, "tp": yy * 2 + c},
        )

    for k in range(chunks):

        def add(zz, carry):
            o_wait(zz, k).wait_recv()
            own_acc[k * sub : (k + 1) * sub, :] += orx[zz, k * sub : (k + 1) * sub, :].astype(F32)
            return carry

        @pl.when(x == 0)
        def _():
            add(z, 0)

        @pl.when(is_low)
        def _():
            add(nz, 0)

        lax.fori_loop(z + 1, lax.select(is_low, jnp.int32(top), jnp.int32(nz)), add, 0)
        fin[rows_of(y, k), :] = own_acc[k * sub : (k + 1) * sub, :].astype(BF16)
        for d in range(1, ny):
            ag_y(d, k).start()

    dvx_copy(0).wait_recv()
    dvw = dvw_acc[wrows(i), :] + dvx_rx[z].astype(F32)
    for d in range(1, nz):
        dv_wait(d).wait_recv()
        dvw = dvw + dvw_rx[d].astype(F32)
    dvw_ref[...] = dvw
    for k in range(chunks):
        for d in range(1, ny):
            ag_y_wait(d, k).wait_recv()
    ag_c = remote(
        fin.at[pl.ds(my_half, half)], fin.at[pl.ds(my_half, half)], acs.at[0], acr.at[0], core_peer
    )
    ag_c_wait = remote(
        fin.at[pl.ds(peer_half, half)], fin.at[pl.ds(peer_half, half)], acs.at[0], acr.at[0], core_peer
    )
    ag_c.start()

    def out_copy(at, k):
        return pltpu.make_async_copy(
            fin.at[pl.ds(at, half), pl.ds(0, latent_dim)], dlat_hbm.at[pl.ds(at, half)], ld.at[k]
        )

    out_copy(my_half, 0).start()

    @pl.when(last > 0)
    def _():
        sends_done(last)

    @pl.when(has_next)
    def _():
        for k in range(parts):
            z_copy(i, k).wait_send()

    @pl.when(jnp.logical_or(x == 0, is_low))
    def _():
        for k in range(parts):
            x_copy(i, k).wait_send()

    @pl.when(is_low)
    def _():
        back_copy().wait_send()

    def drain(n, carry):
        @pl.when(jnp.logical_or(own_column(n), in_plane(n)))
        def _():
            for k in range(chunks):
                o_copy(n, k).wait_send()

        @pl.when(for_x_sum(n))
        def _():
            for k in range(chunks):
                xr_copy(n, k).wait_send()

        @pl.when(visit_out(n))
        def _():
            for k in range(chunks):
                v_copy(n, k).wait_send()

        return carry

    lax.fori_loop(1, last + 1, drain, 0)
    for d in range(1, nz):
        dv_copy(d).wait_send()
    for d in range(nz):
        dvx_copy(d).wait_send()
    for k in range(chunks):
        for d in range(1, ny):
            ag_y(d, k).wait_send()
    ag_c_wait.wait_recv()
    ag_c.wait_send()
    out_copy(peer_half, 1).start()
    drope_ref[...] = fin[:, latent_dim : latent_dim + ROPE].astype(F32).T
    dq_out.wait()
    out_copy(my_half, 0).wait()
    out_copy(peer_half, 1).wait()


def fused_backward(ns, tp, queries, out_grad, attn_out, lse, latent, rope_t, key_weight, value_weight):
    rows = queries.shape[0]
    latent_dim, hv = key_weight.shape
    heads = hv // NOPE
    packed = latent_dim + WIDE - NOPE
    lrows = latent_dim // ns
    ny = tp // 2
    chunks = min(4, rows // tp // 32)
    parts = chunks
    hbm = pl.BlockSpec(memory_space=pl.ANY)
    vmem = pl.BlockSpec(memory_space=pltpu.VMEM)
    dma = pltpu.SemaphoreType.DMA
    return pl.pallas_call(
        functools.partial(fused_kernel, ns, tp, heads, latent_dim),
        in_specs=[hbm, hbm, hbm, vmem, hbm, vmem, hbm, hbm],
        out_specs=[hbm, hbm, vmem, vmem],
        out_shape=[
            jax.ShapeDtypeStruct(queries.shape, BF16),
            jax.ShapeDtypeStruct(latent.shape, BF16),
            jax.ShapeDtypeStruct(rope_t.shape, F32),
            jax.ShapeDtypeStruct((lrows, hv), F32),
        ],
        scratch_shapes=[
            pltpu.VMEM(queries.shape, BF16),
            pltpu.VMEM((2,) + out_grad.shape, BF16),
            pltpu.VMEM(queries.shape, BF16),
            pltpu.VMEM((2, heads, rows), F32),
            pltpu.VMEM(attn_out.shape, BF16),
            pltpu.VMEM(key_weight.shape, BF16),
            pltpu.VMEM(value_weight.shape, BF16),
            pltpu.VMEM((2, heads, rows, WIDE), BF16),
            pltpu.VMEM((2, heads, WIDE, rows), BF16),
            pltpu.VMEM((2, heads, VDIM, rows), BF16),
            pltpu.VMEM((2, heads, NOPE + ROPE, rows), F32),
            pltpu.VMEM((2, heads, rows), F32),
            pltpu.VMEM((heads, rows, WIDE), BF16),
            pltpu.VMEM((heads, NOPE + ROPE, rows), BF16),
            pltpu.VMEM((latent_dim, rows), BF16),
            pltpu.VMEM((rows, hv), BF16),
            pltpu.VMEM((rows, hv), BF16),
            pltpu.VMEM((rows, hv), BF16),
            pltpu.VMEM((latent_dim, hv), F32),
            pltpu.VMEM((2, ns // 2, lrows, hv), BF16),
            pltpu.VMEM((ns // 2, lrows, hv), BF16),
            pltpu.VMEM((ns // 2, lrows, hv), BF16),
            pltpu.VMEM((ns + 2, rows, packed), BF16),
            pltpu.VMEM((ns, rows // 2, packed), BF16),
            pltpu.VMEM((ns, max(ny - 1, 1), rows // tp, packed), BF16),
            pltpu.VMEM((ns, rows // tp, packed), BF16),
            pltpu.VMEM((ns // 2 + 1, rows // tp, packed), BF16),
            pltpu.VMEM((rows // tp, packed), F32),
            pltpu.VMEM((rows, packed), BF16),
            dma((6,)),
            dma((ns, parts)),
            dma((ns, parts)),
            dma((ns, parts)),
            dma((ns, parts)),
            dma((ns, parts)),
            dma((ns, parts)),
            dma((ns, chunks)),
            dma((ns, chunks)),
            dma((ns,)),
            dma((ns,)),
            dma((ns, max(ny - 1, 1), chunks)),
            dma((ns, max(ny - 1, 1), chunks)),
            dma((ns // 2 + 1, chunks)),
            dma((ns, chunks)),
            dma((ns // 2,)),
            dma((ns // 2,)),
            dma((ns // 2,)),
            dma((ns // 2,)),
            dma((max(ny - 1, 1), chunks)),
            dma((max(ny - 1, 1), chunks)),
            dma((1,)),
            dma((1,)),
            dma((5,)),
            dma((5,)),
        ],
        compiler_params=pltpu.CompilerParams(
            collective_id=0, has_side_effects=True, vmem_limit_bytes=67043328
        ),
    )(queries, out_grad, attn_out, lse, latent, rope_t, key_weight, value_weight)


def finish_kernel(dq_ref, dlat_ref, drope_ref, dvw_ref, dq_out, dlat_out, drope_out, dvw_out):
    dq_out[...] = dq_ref[...]
    dlat_out[...] = dlat_ref[...].astype(F32)
    drope_out[...] = drope_ref[...]
    dvw_out[...] = dvw_ref[...]


def finish(dq, dlat, drope_t, dvw):
    steps = 2

    def rows_of(a):
        return pl.BlockSpec((a.shape[0] // steps, a.shape[1]), lambda k: (k, 0))

    specs = [rows_of(a) for a in (dq, dlat, drope_t, dvw)]
    return pl.pallas_call(
        finish_kernel,
        grid=(steps,),
        in_specs=specs,
        out_specs=specs,
        out_shape=[
            jax.ShapeDtypeStruct(dq.shape, BF16),
            jax.ShapeDtypeStruct(dlat.shape, F32),
            jax.ShapeDtypeStruct(drope_t.shape, F32),
            jax.ShapeDtypeStruct(dvw.shape, F32),
        ],
        compiler_params=pltpu.CompilerParams(dimension_semantics=("arbitrary",)),
    )(dq, dlat, drope_t, dvw)


def per_device(queries, latent, rope_key, key_weight, value_weight, log_sums, attn_out, out_grad):
    d_queries, dlat, drope_t, d_value_weight = fused_backward(
        lax.axis_size("sp"), lax.axis_size("tp"),
        queries, out_grad, attn_out, log_sums, latent, rope_key.T, key_weight, value_weight,
    )
    d_queries, d_latent, drope_t, d_value_weight = finish(d_queries, dlat, drope_t, d_value_weight)
    d_rope = drope_t.T
    return (d_queries, d_latent, d_rope, d_value_weight)


def solution(mesh):
    placed = (
        P("sp", "tp"),
        P("sp", None),
        P("sp", None),
        P(None, "tp"),
        P(None, "tp"),
        P("tp", "sp"),
        P("sp", "tp"),
        P("sp", "tp"),
    )
    return jax.shard_map(
        per_device,
        mesh=mesh,
        in_specs=placed,
        out_specs=(P("sp", "tp"), P("sp", None), P("sp", None), P("sp", "tp")),
        check_vma=False,
    )
```

```python
import functools

import jax
import jax.numpy as jnp
from jax import lax
from jax.experimental import pallas as pl
from jax.experimental.pallas import tpu as pltpu
from jax.sharding import PartitionSpec as P

NOPE = 128
ROPE = 64
VDIM = 128
WIDE = 256
LOG2E = 1.4426950408889634
BF16 = jnp.bfloat16
F32 = jnp.float32
MESH = pl.DeviceIdType.MESH


def dot_nn(a, b):
    return lax.dot_general(a, b, (((1,), (0,)), ((), ())), preferred_element_type=F32)


def dot_nt(a, b):
    return lax.dot_general(a, b, (((1,), (1,)), ((), ())), preferred_element_type=F32)


def fused_kernel(
    ns,
    tp,
    heads,
    latent_dim,
    q_hbm,
    g_hbm,
    ao_hbm,
    lse_ref,
    lat_hbm,
    rope_ref,
    wk_hbm,
    wv_hbm,
    dq_hbm,
    dlat_hbm,
    drope_hbm,
    dvw_hbm,
    q_v,
    g_v,
    fq_v,
    lse_s,
    ao_v,
    wk_v,
    wv_v,
    qs_s,
    qt_s,
    gt_s,
    dqt_s,
    delta_s,
    kc_s,
    kct_s,
    lat_t,
    v_s,
    dk_s,
    dv_s,
    dvw_acc,
    dvw_b,
    dvx_rx,
    dvw_rx,
    lat_all,
    crx,
    yrx,
    xrx,
    orx,
    own_acc,
    fin,
    dvw_o,
    drope_o,
    ld,
    zr,
    zs,
    xr,
    xs,
    cr,
    cs,
    xrr,
    xrs,
    r1r,
    r1s,
    yr,
    ys,
    orr,
    ors,
    dvr,
    dvs,
    dvxr,
    dvxs,
    agr,
    ags,
    acr,
    acs,
    vr,
    vs,
):
    i = lax.axis_index("sp")
    t = lax.axis_index("tp")
    ny = tp // 2
    nz = ns // 2
    z, x = i // 2, i % 2
    y, c = t // 2, t % 2
    rows, width = q_v.shape[0], NOPE + ROPE
    half, piece = rows // 2, rows // tp
    parts = zr.shape[1]
    bit = half // parts
    early, late = range(parts // 2), range(parts // 2, parts)
    scale = width ** (-0.5)
    lrows = latent_dim // ns
    chunks = yr.shape[2]
    sub = piece // chunks

    top = nz - 1
    is_top, is_low = z == top, z == 0
    lower = lax.select(is_top, 2 * (z - 1), 2 * z)
    base = lower + x
    last = base + lax.select(is_low, jnp.int32(2), jnp.int32(0))

    def visiting(n):
        return n > base

    def block_of(n):
        down = 2 * (z - 1 - (n - 1) // 2) + (x + n - 1) % 2
        home = lax.select(n == 0, i, lax.select(n > lower, jnp.int32(2 * z), down))
        return lax.select(visiting(n), lax.select(n == base + 1, i, 1 - i), home)

    def key_of(n):
        return lax.select(visiting(n), block_of(n) + 2, block_of(n))

    def part_of(n):
        later = lax.select(is_low, n, block_of(n - 1))
        return lax.select(n == 0, jnp.int32(ns), lax.select(n == 1, jnp.int32(ns + 1), later))

    def own_column(n):
        return jnp.logical_and(n % 2 == 1, n <= lower)

    def for_x_sum(n):
        return jnp.logical_and(jnp.logical_and(n >= 1, n <= lower), n % 2 == 0)

    def in_plane(n):
        return jnp.logical_and(x == 1, n == lower + 1)

    def by_x(n):
        mine = jnp.logical_and(is_low, jnp.logical_and(x == 0, n == base + 2))
        return jnp.logical_or(for_x_sum(n), jnp.logical_or(in_plane(n), mine))

    def visit_out(n):
        return jnp.logical_and(is_low, n == base + 2)

    my_half = pl.multiple_of(c * half, half)
    peer_half = pl.multiple_of((1 - c) * half, half)
    core_peer = {"sp": i, "tp": y * 2 + 1 - c}
    x_peer = {"sp": 2 * z + 1 - x, "tp": t}
    above = {"sp": lax.min(i + 2, ns - 1), "tp": t}

    def remote(src, dst, ssem, rsem, dev):
        return pltpu.make_async_remote_copy(
            src_ref=src, dst_ref=dst, send_sem=ssem, recv_sem=rsem, device_id=dev, device_id_type=MESH
        )

    def lat_rows(j, at, size):
        return lat_all.at[j, pl.ds(at, size)]

    own_cps = [pltpu.make_async_copy(lat_hbm, lat_all.at[i, :, pl.ds(0, latent_dim)], ld.at[0])]
    loads = [
        pltpu.make_async_copy(s, d, ld.at[k + 1])
        for k, (s, d) in enumerate(
            ((g_hbm, g_v.at[0]), (q_hbm, q_v), (ao_hbm, ao_v), (wk_hbm, wk_v), (wv_hbm, wv_v))
        )
    ]
    for cp in own_cps + loads:
        cp.start()

    lat_all[i, :, latent_dim:] = jnp.concatenate(
        [rope_ref[...].T, jnp.zeros((rows, WIDE - NOPE - ROPE), BF16)], axis=1
    )

    barrier = pltpu.get_barrier_semaphore()
    for d in range(1, ns):
        pl.semaphore_signal(
            barrier, inc=1, device_id={"sp": (i + d) % ns, "tp": t}, device_id_type=MESH
        )
    for d in range(1, tp):
        pl.semaphore_signal(
            barrier, inc=1, device_id={"sp": i, "tp": (t + d) % tp}, device_id_type=MESH
        )
    pl.semaphore_wait(barrier, ns - 1 + tp - 1)
    for cp in own_cps:
        cp.wait()

    def bit_of(j, k):
        return lat_rows(j, pl.multiple_of(c * half + k * bit, bit), bit)

    def pair_of(j):
        return lax.select(j // 2 == z, jnp.int32(2), (z + nz - 1 - j // 2) % 2)

    def z_copy(j, k):
        return remote(bit_of(j, k), bit_of(j, k), zs.at[pair_of(j), k], zr.at[j // 2, k], above)

    def x_copy(j, k):
        return remote(bit_of(j, k), bit_of(j, k), xs.at[pair_of(j), k], xr.at[j // 2, k], x_peer)

    def c_copy(n, k):
        j = block_of(n)
        return remote(bit_of(j, k), bit_of(j, k), cs.at[n % 4, k], cr.at[n % 4, k], core_peer)

    has_next = z + 1 < nz

    @pl.when(has_next)
    def _():
        for k in range(parts):
            z_copy(i, k).start()

    @pl.when(jnp.logical_or(x == 0, is_low))
    def _():
        for k in early:
            x_copy(i, k).start()

    @pl.when(is_low)
    def _():
        for k in late:
            x_copy(i, k).start()

    def goes_on(n):
        return jnp.logical_and(has_next, jnp.logical_or(z + 1 != top, block_of(n) >= 2))

    low_peer = {"sp": x, "tp": t}
    top_peer = {"sp": 2 * top + x, "tp": t}

    visits = ((g_v.at[0], g_v.at[1]), (q_v, fq_v), (lse_ref, lse_s.at[1]), (delta_s.at[0], delta_s.at[1]))

    def visit_copy(k):
        return remote(visits[k][0], visits[k][1], vs.at[k], vr.at[k], low_peer)

    def back_copy():
        return remote(fq_v, fq_v, vs.at[4], vr.at[4], top_peer)

    def stage_a(n, pieces):
        @pl.when(own_column(n))
        def _():
            j = block_of(n)
            for k in pieces:
                z_copy(j, k).wait_recv()
                x_copy(j, k).start()
                c_copy(n, k).start()

                @pl.when(goes_on(n))
                def _():
                    z_copy(j, k).start()

    def stage_b(n):
        j = block_of(n)
        for k in range(parts):
            x_copy(j, k).wait_recv()
            c_copy(n, k).start()

    def sends_done(n):
        j = block_of(n)

        @pl.when(jnp.logical_or(own_column(n), by_x(n)))
        def _():
            for k in range(parts):
                c_copy(n, k).wait_send()

        @pl.when(own_column(n))
        def _():
            for k in range(parts):
                x_copy(j, k).wait_send()

            @pl.when(goes_on(n))
            def _():
                for k in range(parts):
                    z_copy(j, k).wait_send()

    def r1_copy(n):
        j = key_of(n)
        return remote(
            lat_rows(part_of(n), peer_half, half), crx.at[j], r1s.at[j], r1r.at[j], core_peer
        )

    def rows_of(yy, k):
        return pl.ds(pl.multiple_of(c * half + yy * piece + k * sub, sub), sub)

    def chunk(k):
        return pl.ds(k * sub, sub)

    def y_copy(n, d, k):
        j = key_of(n)
        yy = (y + d) % ny
        return remote(
            lat_all.at[part_of(n), rows_of(yy, k)], yrx.at[j, d - 1, chunk(k)],
            ys.at[n % 4, d - 1, k], yr.at[n % 4, d - 1, k], {"sp": i, "tp": yy * 2 + c},
        )

    def xr_copy(n, k):
        j = block_of(n)
        return remote(
            lat_all.at[part_of(n), rows_of(y, k)], xrx.at[j, chunk(k)], xrs.at[j // 2, k],
            xrr.at[j // 2, k], x_peer,
        )

    def o_copy(n, k):
        return remote(
            lat_all.at[part_of(n), rows_of(y, k)], orx.at[z, chunk(k)], ors.at[block_of(n) // 2, k],
            orr.at[z, k],
            {"sp": block_of(n), "tp": t},
        )

    def v_copy(n, k):
        return remote(
            lat_all.at[part_of(n), rows_of(y, k)], orx.at[nz, chunk(k)], ors.at[1, k],
            orr.at[nz, k], x_peer,
        )

    def o_wait(zz, k):
        return remote(
            lat_all.at[i, rows_of(y, k)], orx.at[zz, chunk(k)], ors.at[0, k], orr.at[zz, k], x_peer
        )

    def stage_r2(n):
        j = key_of(n)
        b = part_of(n)
        r1_copy(n).wait_recv()

        def add_core(yy, k):
            at = pl.ds(pl.multiple_of(yy * piece + k * sub, sub), sub)
            lat_all[b, rows_of(yy, k), :] = lat_all[b, rows_of(yy, k), :] + crx[j, at, :]

        for k in range(chunks):
            for d in range(1, ny):
                add_core((y + d) % ny, k)
                y_copy(n, d, k).start()
        for k in range(chunks):
            add_core(y, k)

    def stage_r3(n):
        j = key_of(n)
        b = part_of(n)
        for k in range(chunks):
            total = lat_all[b, rows_of(y, k), :].astype(F32)
            for d in range(1, ny):
                y_copy(n, d, k).wait_recv()
                total = total + yrx[j, d - 1, k * sub : (k + 1) * sub, :].astype(F32)

            @pl.when(n == 0)
            def _():
                own_acc[k * sub : (k + 1) * sub, :] = total

            @pl.when(jnp.logical_and(is_low, n == base + 1))
            def _():
                own_acc[k * sub : (k + 1) * sub, :] += total

            @pl.when(n > 0)
            def _():
                lat_all[b, rows_of(y, k), :] = total.astype(BF16)

            @pl.when(for_x_sum(n))
            def _():
                xr_copy(n, k).start()

            @pl.when(in_plane(n))
            def _():
                o_copy(n, k).start()

            @pl.when(visit_out(n))
            def _():
                v_copy(n, k).start()

        for k in range(chunks):
            for d in range(1, ny):
                y_copy(n, d, k).wait_send()
        r1_copy(n).wait_send()

    def stage_r4(n):
        @pl.when(own_column(n))
        def _():
            j = block_of(n)
            b = part_of(n)
            for k in range(chunks):
                xr_copy(n, k).wait_recv()
                total = (
                    lat_all[b, rows_of(y, k), :].astype(F32)
                    + xrx[j, k * sub : (k + 1) * sub, :].astype(F32)
                )
                lat_all[b, rows_of(y, k), :] = total.astype(BF16)
                o_copy(n, k).start()

    def prepare(qi, q_ref):
        for h in range(heads):
            qh = jnp.concatenate(
                [q_ref[:, h * width : (h + 1) * width], jnp.zeros((rows, WIDE - width), BF16)], axis=1
            )
            qs_s[qi, h] = qh
            qt_s[qi, h] = qh.T
            gt_s[qi, h] = g_v[qi, :, h * VDIM : (h + 1) * VDIM].T
        dqt_s[qi] = jnp.zeros_like(dqt_s[qi])

    for cp in loads[:2]:
        cp.wait()

    @pl.when(is_top)
    def _():
        for k in range(3):
            visit_copy(k).start()

    for cp in loads[2:]:
        cp.wait()
    prepare(0, q_v)
    for h in range(heads):
        at = ao_v[:, h * VDIM : (h + 1) * VDIM].T
        delta_s[0, h : h + 1, :] = jnp.sum(
            gt_s[0, h].astype(F32) * at.astype(F32), axis=0, keepdims=True
        )
    lse_s[0] = lse_ref[...]

    @pl.when(is_top)
    def _():
        visit_copy(3).start()

    dvw_acc[...] = jnp.zeros_like(dvw_acc)

    def slot(n, diagonal):
        j = block_of(n)
        b = part_of(n)
        qi = lax.select(visiting(n), jnp.int32(1), jnp.int32(0))

        if not diagonal:

            @pl.when(jnp.logical_or(own_column(n), by_x(n)))
            def _():
                for k in range(parts):
                    c_copy(n, k).wait_recv()

            @pl.when(n == base + 1)
            def _():
                for k in range(4):
                    visit_copy(k).wait_recv()
                prepare(1, fq_v)

        rope = lat_all[j, :, latent_dim:]
        rope_t = rope.T[:ROPE]
        lat_t[...] = lat_all[j, :, :latent_dim].T
        keys = dot_nn(lat_all[j, :, :latent_dim], wk_v[...]).astype(BF16)
        v_s[...] = dot_nn(lat_all[j, :, :latent_dim], wv_v[...]).astype(BF16)
        for h in range(heads):
            kc = jnp.concatenate([keys[:, h * NOPE : (h + 1) * NOPE], rope], axis=1)
            kc_s[h] = kc
            kct_s[h, :NOPE] = keys[:, h * NOPE : (h + 1) * NOPE].T
            kct_s[h, NOPE:] = rope_t
        rope_sum = jnp.zeros((rows, WIDE - NOPE), F32)
        for h in range(heads):
            s = dot_nn(kc_s[h], qt_s[qi, h])
            zz = s * (scale * LOG2E) - lse_s[qi, h : h + 1, :] * LOG2E
            if diagonal:
                k_pos = lax.broadcasted_iota(jnp.int32, (rows, rows), 0)
                q_pos = lax.broadcasted_iota(jnp.int32, (rows, rows), 1)
                zz = jnp.where(k_pos <= q_pos, zz, -1e30)
            p = jnp.exp2(zz)
            dp = dot_nn(v_s[:, h * VDIM : (h + 1) * VDIM], gt_s[qi, h])
            ds = (p * (dp - delta_s[qi, h : h + 1, :])).astype(BF16)
            dv_s[:, h * VDIM : (h + 1) * VDIM] = dot_nn(
                p.astype(BF16), g_v[qi, :, h * VDIM : (h + 1) * VDIM]
            ).astype(BF16)
            dk = scale * dot_nn(ds, qs_s[qi, h])
            dk_s[:, h * NOPE : (h + 1) * NOPE] = dk[:, :NOPE].astype(BF16)
            rope_sum = rope_sum + dk[:, NOPE:]
            dqt_s[qi, h] += dot_nn(kct_s[h], ds)
            if h == heads // 2 - 1 and not diagonal:
                stage_r2(n - 1)

                @pl.when(n > 1)
                def _():
                    stage_a(n + 1, late)

        if not diagonal:

            @pl.when(n > 1)
            def _():
                stage_r3(n - 2)
                sends_done(n - 1)

                @pl.when(n > 4)
                def _():
                    stage_r4(n - 4)

                @pl.when(in_plane(n + 1))
                def _():
                    stage_b(n + 1)

        dlat = dot_nt(dk_s[...], wk_v[...]) + dot_nt(dv_s[...], wv_v[...])
        lat_all[b, :, :latent_dim] = dlat.astype(BF16)
        lat_all[b, :, latent_dim:] = rope_sum.astype(BF16)
        r1_copy(n).start()

        if diagonal:
            stage_a(n + 1, range(parts))

        @pl.when(jnp.logical_and(by_x(n + 1), jnp.logical_or(is_low, jnp.logical_not(in_plane(n + 1)))))
        def _():
            stage_b(n + 1)

        dvw_acc[...] += dot_nn(lat_t[...], dv_s[...])

        if not diagonal:
            stage_a(n + 2, early)

            @pl.when(jnp.logical_and(jnp.logical_and(x == 0, z > 0), n == 2))
            def _():
                for k in late:
                    x_copy(i, k).start()

    slot(jnp.int32(0), True)

    def later_slot(n, carry):
        slot(n, False)
        return carry

    lax.fori_loop(1, last + 1, later_slot, 0)

    @pl.when(is_low)
    def _():
        for h in range(heads):
            fq_v[:, h * width : (h + 1) * width] = (scale * dqt_s[1, h]).T.astype(BF16)
        back_copy().start()

    def wrows(k):
        return pl.ds(pl.multiple_of(k * lrows, lrows), lrows)

    def dvx_copy(d):
        zz = (z + d) % nz
        return remote(dvw_b.at[1 - x, zz], dvx_rx.at[zz], dvxs.at[d], dvxr.at[d], x_peer)

    send_order = tuple(range(1, nz)) + (0,)

    def dv_copy(d):
        zz = (z + d) % nz
        return remote(
            dvw_b.at[x, zz], dvw_rx.at[nz - d], dvs.at[d], dvr.at[nz - d], {"sp": 2 * zz + x, "tp": t}
        )

    def dv_wait(d):
        return remote(dvw_b.at[x, z], dvw_rx.at[d], dvs.at[d], dvr.at[d], x_peer)

    for k in range(ns):
        dvw_b[k % 2, k // 2] = dvw_acc[k * lrows : (k + 1) * lrows, :].astype(BF16)

    stage_r2(last)

    @pl.when(last > 3)
    def _():
        stage_r4(last - 3)

    @pl.when(last > 0)
    def _():
        stage_r3(last - 1)

    @pl.when(x == 1)
    def _():
        for d in send_order:
            dvx_copy(d).start()

    @pl.when(jnp.logical_and(x == 1, last > 2))
    def _():
        stage_r4(last - 2)

    @pl.when(jnp.logical_not(is_top))
    def _():
        for h in range(heads):
            q_v[:, h * width : (h + 1) * width] = (
                (scale * dqt_s[0, h]).T.astype(BF16)
            )

    stage_r3(last)

    @pl.when(x == 0)
    def _():
        for d in send_order:
            dvx_copy(d).start()

    def tail(n, carry):
        stage_r4(n)
        return carry

    lax.fori_loop(lax.max(last - 2 + x, 1), lower + 1, tail, 0)
    for d in range(1, nz):
        dvx_copy(d).wait_recv()
        zz = (z + d) % nz
        dvw_b[x, zz] = (dvw_acc[wrows(2 * zz + x), :] + dvx_rx[zz].astype(F32)).astype(BF16)
        dv_copy(d).start()

    @pl.when(is_top)
    def _():
        for k in range(4):
            visit_copy(k).wait_send()
        back_copy().wait_recv()
        for h in range(heads):
            q_v[:, h * width : (h + 1) * width] = (
                (scale * dqt_s[0, h]).T
                + fq_v[:, h * width : (h + 1) * width].astype(F32)
            ).astype(BF16)

    dq_out = pltpu.make_async_copy(q_v, dq_hbm, ld.at[2])
    dq_out.start()

    def ag_y(d, k):
        yy = (y + d) % ny
        return remote(
            fin.at[rows_of(y, k)], fin.at[rows_of(y, k)], ags.at[d - 1, k], agr.at[d - 1, k],
            {"sp": i, "tp": yy * 2 + c},
        )

    def ag_y_wait(d, k):
        yy = (y + ny - d) % ny
        return remote(
            fin.at[rows_of(yy, k)], fin.at[rows_of(yy, k)], ags.at[d - 1, k], agr.at[d - 1, k],
            {"sp": i, "tp": yy * 2 + c},
        )

    for k in range(chunks):

        def add(zz, carry):
            o_wait(zz, k).wait_recv()
            own_acc[k * sub : (k + 1) * sub, :] += orx[zz, k * sub : (k + 1) * sub, :].astype(F32)
            return carry

        @pl.when(x == 0)
        def _():
            add(z, 0)

        @pl.when(is_low)
        def _():
            add(nz, 0)

        lax.fori_loop(z + 1, lax.select(is_low, jnp.int32(top), jnp.int32(nz)), add, 0)
        fin[rows_of(y, k), :] = own_acc[k * sub : (k + 1) * sub, :].astype(BF16)
        for d in range(1, ny):
            ag_y(d, k).start()

    for k in range(chunks):
        for d in range(1, ny):
            ag_y_wait(d, k).wait_recv()
    ag_c = remote(
        fin.at[pl.ds(my_half, half)], fin.at[pl.ds(my_half, half)], acs.at[0], acr.at[0], core_peer
    )
    ag_c_wait = remote(
        fin.at[pl.ds(peer_half, half)], fin.at[pl.ds(peer_half, half)], acs.at[0], acr.at[0], core_peer
    )
    ag_c.start()

    def out_copy(at, k):
        return pltpu.make_async_copy(
            fin.at[pl.ds(at, half), pl.ds(0, latent_dim)], dlat_hbm.at[pl.ds(at, half)], ld.at[k]
        )

    out_copy(my_half, 0).start()
    dvx_copy(0).wait_recv()
    dvw = dvw_acc[wrows(i), :] + dvx_rx[z].astype(F32)
    for d in range(1, nz):
        dv_wait(d).wait_recv()
        dvw = dvw + dvw_rx[d].astype(F32)
    dvw_o[...] = dvw
    dvw_out = pltpu.make_async_copy(dvw_o, dvw_hbm, ld.at[3])
    dvw_out.start()

    @pl.when(last > 0)
    def _():
        sends_done(last)

    @pl.when(has_next)
    def _():
        for k in range(parts):
            z_copy(i, k).wait_send()

    @pl.when(jnp.logical_or(x == 0, is_low))
    def _():
        for k in range(parts):
            x_copy(i, k).wait_send()

    @pl.when(is_low)
    def _():
        back_copy().wait_send()

    def drain(n, carry):
        @pl.when(jnp.logical_or(own_column(n), in_plane(n)))
        def _():
            for k in range(chunks):
                o_copy(n, k).wait_send()

        @pl.when(for_x_sum(n))
        def _():
            for k in range(chunks):
                xr_copy(n, k).wait_send()

        @pl.when(visit_out(n))
        def _():
            for k in range(chunks):
                v_copy(n, k).wait_send()

        return carry

    lax.fori_loop(1, last + 1, drain, 0)
    for d in range(1, nz):
        dv_copy(d).wait_send()
    for d in range(nz):
        dvx_copy(d).wait_send()
    for k in range(chunks):
        for d in range(1, ny):
            ag_y(d, k).wait_send()
    ag_c_wait.wait_recv()
    out_copy(peer_half, 1).start()
    drope_o[...] = fin[:, latent_dim : latent_dim + ROPE].astype(F32).T
    drope_out = pltpu.make_async_copy(drope_o, drope_hbm, ld.at[4])
    drope_out.start()
    ag_c.wait_send()
    with jax.named_scope("outs"):
        dq_out.wait()
        dvw_out.wait()
        out_copy(my_half, 0).wait()
        out_copy(peer_half, 1).wait()
        drope_out.wait()


def fused_backward(ns, tp, queries, out_grad, attn_out, lse, latent, rope_t, key_weight, value_weight):
    rows = queries.shape[0]
    latent_dim, hv = key_weight.shape
    heads = hv // NOPE
    packed = latent_dim + WIDE - NOPE
    lrows = latent_dim // ns
    ny = tp // 2
    chunks = min(4, rows // tp // 32)
    parts = chunks
    hbm = pl.BlockSpec(memory_space=pl.ANY)
    vmem = pl.BlockSpec(memory_space=pltpu.VMEM)
    dma = pltpu.SemaphoreType.DMA
    return pl.pallas_call(
        functools.partial(fused_kernel, ns, tp, heads, latent_dim),
        in_specs=[hbm, hbm, hbm, vmem, hbm, vmem, hbm, hbm],
        out_specs=[hbm, hbm, hbm, hbm],
        out_shape=[
            jax.ShapeDtypeStruct(queries.shape, BF16),
            jax.ShapeDtypeStruct(latent.shape, BF16),
            jax.ShapeDtypeStruct(rope_t.shape, F32),
            jax.ShapeDtypeStruct((lrows, hv), F32),
        ],
        scratch_shapes=[
            pltpu.VMEM(queries.shape, BF16),
            pltpu.VMEM((2,) + out_grad.shape, BF16),
            pltpu.VMEM(queries.shape, BF16),
            pltpu.VMEM((2, heads, rows), F32),
            pltpu.VMEM(attn_out.shape, BF16),
            pltpu.VMEM(key_weight.shape, BF16),
            pltpu.VMEM(value_weight.shape, BF16),
            pltpu.VMEM((2, heads, rows, WIDE), BF16),
            pltpu.VMEM((2, heads, WIDE, rows), BF16),
            pltpu.VMEM((2, heads, VDIM, rows), BF16),
            pltpu.VMEM((2, heads, NOPE + ROPE, rows), F32),
            pltpu.VMEM((2, heads, rows), F32),
            pltpu.VMEM((heads, rows, WIDE), BF16),
            pltpu.VMEM((heads, NOPE + ROPE, rows), BF16),
            pltpu.VMEM((latent_dim, rows), BF16),
            pltpu.VMEM((rows, hv), BF16),
            pltpu.VMEM((rows, hv), BF16),
            pltpu.VMEM((rows, hv), BF16),
            pltpu.VMEM((latent_dim, hv), F32),
            pltpu.VMEM((2, ns // 2, lrows, hv), BF16),
            pltpu.VMEM((ns // 2, lrows, hv), BF16),
            pltpu.VMEM((ns // 2, lrows, hv), BF16),
            pltpu.VMEM((ns + 2, rows, packed), BF16),
            pltpu.VMEM((ns, rows // 2, packed), BF16),
            pltpu.VMEM((ns, max(ny - 1, 1), rows // tp, packed), BF16),
            pltpu.VMEM((ns, rows // tp, packed), BF16),
            pltpu.VMEM((ns // 2 + 1, rows // tp, packed), BF16),
            pltpu.VMEM((rows // tp, packed), F32),
            pltpu.VMEM((rows, packed), BF16),
            pltpu.VMEM((lrows, hv), F32),
            pltpu.VMEM(rope_t.shape, F32),
            dma((6,)),
            dma((ns // 2, parts)),
            dma((3, parts)),
            dma((ns // 2, parts)),
            dma((3, parts)),
            dma((4, parts)),
            dma((4, parts)),
            dma((ns // 2, chunks)),
            dma((ns // 2, chunks)),
            dma((ns,)),
            dma((ns,)),
            dma((4, max(ny - 1, 1), chunks)),
            dma((4, max(ny - 1, 1), chunks)),
            dma((ns // 2 + 1, chunks)),
            dma((ns // 2, chunks)),
            dma((ns // 2,)),
            dma((ns // 2,)),
            dma((ns // 2,)),
            dma((ns // 2,)),
            dma((max(ny - 1, 1), chunks)),
            dma((max(ny - 1, 1), chunks)),
            dma((1,)),
            dma((1,)),
            dma((5,)),
            dma((5,)),
        ],
        compiler_params=pltpu.CompilerParams(
            collective_id=0, has_side_effects=True, vmem_limit_bytes=67043328
        ),
    )(queries, out_grad, attn_out, lse, latent, rope_t, key_weight, value_weight)


def finish_kernel(dq_ref, dlat_ref, drope_ref, dvw_ref, dq_out, dlat_out, drope_out, dvw_out):
    dq_out[...] = dq_ref[...]
    dlat_out[...] = dlat_ref[...].astype(F32)
    drope_out[...] = drope_ref[...]
    dvw_out[...] = dvw_ref[...]


def finish(dq, dlat, drope_t, dvw):
    steps = 2

    def rows_of(a):
        return pl.BlockSpec((a.shape[0] // steps, a.shape[1]), lambda k: (k, 0))

    specs = [rows_of(a) for a in (dq, dlat, drope_t, dvw)]
    return pl.pallas_call(
        finish_kernel,
        grid=(steps,),
        in_specs=specs,
        out_specs=specs,
        out_shape=[
            jax.ShapeDtypeStruct(dq.shape, BF16),
            jax.ShapeDtypeStruct(dlat.shape, F32),
            jax.ShapeDtypeStruct(drope_t.shape, F32),
            jax.ShapeDtypeStruct(dvw.shape, F32),
        ],
        compiler_params=pltpu.CompilerParams(dimension_semantics=("arbitrary",)),
    )(dq, dlat, drope_t, dvw)


def per_device(queries, latent, rope_key, key_weight, value_weight, log_sums, attn_out, out_grad):
    d_queries, dlat, drope_t, d_value_weight = fused_backward(
        lax.axis_size("sp"), lax.axis_size("tp"),
        queries, out_grad, attn_out, log_sums, latent, rope_key.T, key_weight, value_weight,
    )
    d_queries, d_latent, drope_t, d_value_weight = finish(d_queries, dlat, drope_t, d_value_weight)
    d_rope = drope_t.T
    return (d_queries, d_latent, d_rope, d_value_weight)


def solution(mesh):
    placed = (
        P("sp", "tp"),
        P("sp", None),
        P("sp", None),
        P(None, "tp"),
        P(None, "tp"),
        P("tp", "sp"),
        P("sp", "tp"),
        P("sp", "tp"),
    )
    return jax.shard_map(
        per_device,
        mesh=mesh,
        in_specs=placed,
        out_specs=(P("sp", "tp"), P("sp", None), P("sp", None), P("sp", "tp")),
        check_vma=False,
    )
```

```python
import functools

import jax
import jax.numpy as jnp
from jax import lax
from jax.experimental import pallas as pl
from jax.experimental.pallas import tpu as pltpu
from jax.sharding import PartitionSpec as P

NOPE = 128
ROPE = 64
VDIM = 128
WIDE = 256
LOG2E = 1.4426950408889634
BF16 = jnp.bfloat16
F32 = jnp.float32
MESH = pl.DeviceIdType.MESH


def dot_nn(a, b):
    return lax.dot_general(a, b, (((1,), (0,)), ((), ())), preferred_element_type=F32)


def dot_nt(a, b):
    return lax.dot_general(a, b, (((1,), (1,)), ((), ())), preferred_element_type=F32)


def fused_kernel(
    ns,
    tp,
    heads,
    latent_dim,
    q_hbm,
    g_hbm,
    ao_hbm,
    lse_ref,
    lat_hbm,
    rope_ref,
    wk_hbm,
    wv_hbm,
    dq_hbm,
    dlat_hbm,
    drope_hbm,
    dvw_hbm,
    q_v,
    g_v,
    fq_v,
    lse_s,
    ao_v,
    wk_v,
    wv_v,
    qs_s,
    qt_s,
    gt_s,
    dqt_s,
    delta_s,
    kc_s,
    kct_s,
    lat_t,
    v_s,
    dk_s,
    dv_s,
    dvw_acc,
    dvw_b,
    dvx_rx,
    dvw_rx,
    lat_all,
    crx,
    yrx,
    xrx,
    orx,
    own_acc,
    fin,
    dvw_o,
    drope_o,
    ld,
    zr,
    zs,
    xr,
    xs,
    cr,
    cs,
    xrr,
    xrs,
    r1r,
    r1s,
    yr,
    ys,
    orr,
    ors,
    dvr,
    dvs,
    dvxr,
    dvxs,
    agr,
    ags,
    acr,
    acs,
    vr,
    vs,
):
    i = lax.axis_index("sp")
    t = lax.axis_index("tp")
    ny = tp // 2
    nz = ns // 2
    z, x = i // 2, i % 2
    y, c = t // 2, t % 2
    rows, width = q_v.shape[0], NOPE + ROPE
    half, piece = rows // 2, rows // tp
    parts = zr.shape[1]
    bit = half // parts
    early, late = range(parts // 2), range(parts // 2, parts)
    scale = width ** (-0.5)
    lrows = latent_dim // ns
    chunks = yr.shape[2]
    sub = piece // chunks

    top = nz - 1
    is_top, is_low = z == top, z == 0
    lower = lax.select(is_top, 2 * (z - 1), 2 * z)
    base = lower + x
    last = base + lax.select(is_low, jnp.int32(2), jnp.int32(0))

    def visiting(n):
        return n > base

    def block_of(n):
        down = 2 * (z - 1 - (n - 1) // 2) + (x + n - 1) % 2
        home = lax.select(n == 0, i, lax.select(n > lower, jnp.int32(2 * z), down))
        return lax.select(visiting(n), lax.select(n == base + 1, i, 1 - i), home)

    def key_of(n):
        return lax.select(visiting(n), block_of(n) + 2, block_of(n))

    def part_of(n):
        later = lax.select(is_low, n, block_of(n - 1))
        return lax.select(n == 0, jnp.int32(ns), lax.select(n == 1, jnp.int32(ns + 1), later))

    def own_column(n):
        return jnp.logical_and(n % 2 == 1, n <= lower)

    def for_x_sum(n):
        return jnp.logical_and(jnp.logical_and(n >= 1, n <= lower), n % 2 == 0)

    def in_plane(n):
        return jnp.logical_and(x == 1, n == lower + 1)

    def by_x(n):
        mine = jnp.logical_and(is_low, jnp.logical_and(x == 0, n == base + 2))
        return jnp.logical_or(for_x_sum(n), jnp.logical_or(in_plane(n), mine))

    def visit_out(n):
        return jnp.logical_and(is_low, n == base + 2)

    my_half = pl.multiple_of(c * half, half)
    peer_half = pl.multiple_of((1 - c) * half, half)
    core_peer = {"sp": i, "tp": y * 2 + 1 - c}
    x_peer = {"sp": 2 * z + 1 - x, "tp": t}
    above = {"sp": lax.min(i + 2, ns - 1), "tp": t}

    def remote(src, dst, ssem, rsem, dev):
        return pltpu.make_async_remote_copy(
            src_ref=src, dst_ref=dst, send_sem=ssem, recv_sem=rsem, device_id=dev, device_id_type=MESH
        )

    def lat_rows(j, at, size):
        return lat_all.at[j, pl.ds(at, size)]

    own_cps = [pltpu.make_async_copy(lat_hbm, lat_all.at[i, :, pl.ds(0, latent_dim)], ld.at[0])]
    loads = [
        pltpu.make_async_copy(s, d, ld.at[k + 1])
        for k, (s, d) in enumerate(
            ((g_hbm, g_v.at[0]), (q_hbm, q_v), (ao_hbm, ao_v), (wk_hbm, wk_v), (wv_hbm, wv_v))
        )
    ]
    for cp in own_cps + loads:
        cp.start()

    lat_all[i, :, latent_dim:] = jnp.concatenate(
        [rope_ref[...].T, jnp.zeros((rows, WIDE - NOPE - ROPE), BF16)], axis=1
    )

    barrier = pltpu.get_barrier_semaphore()
    for d in range(1, ns):
        pl.semaphore_signal(
            barrier, inc=1, device_id={"sp": (i + d) % ns, "tp": t}, device_id_type=MESH
        )
    for d in range(1, tp):
        pl.semaphore_signal(
            barrier, inc=1, device_id={"sp": i, "tp": (t + d) % tp}, device_id_type=MESH
        )
    pl.semaphore_wait(barrier, ns - 1 + tp - 1)
    for cp in own_cps:
        cp.wait()

    def bit_of(j, k):
        return lat_rows(j, pl.multiple_of(c * half + k * bit, bit), bit)

    def pair_of(j):
        return lax.select(j // 2 == z, jnp.int32(2), (z + nz - 1 - j // 2) % 2)

    def z_copy(j, k):
        return remote(bit_of(j, k), bit_of(j, k), zs.at[pair_of(j), k], zr.at[j // 2, k], above)

    def x_copy(j, k):
        return remote(bit_of(j, k), bit_of(j, k), xs.at[pair_of(j), k], xr.at[j // 2, k], x_peer)

    def c_copy(n, k):
        j = block_of(n)
        return remote(bit_of(j, k), bit_of(j, k), cs.at[n % 4, k], cr.at[n % 4, k], core_peer)

    has_next = z + 1 < nz

    @pl.when(has_next)
    def _():
        for k in range(parts):
            z_copy(i, k).start()

    @pl.when(jnp.logical_or(x == 0, is_low))
    def _():
        for k in early:
            x_copy(i, k).start()

    @pl.when(is_low)
    def _():
        for k in late:
            x_copy(i, k).start()

    def goes_on(n):
        return jnp.logical_and(has_next, jnp.logical_or(z + 1 != top, block_of(n) >= 2))

    low_peer = {"sp": x, "tp": t}
    top_peer = {"sp": 2 * top + x, "tp": t}

    visits = ((g_v.at[0], g_v.at[1]), (q_v, fq_v), (lse_ref, lse_s.at[1]), (delta_s.at[0], delta_s.at[1]))

    def visit_copy(k):
        return remote(visits[k][0], visits[k][1], vs.at[k], vr.at[k], low_peer)

    def back_copy():
        return remote(fq_v, fq_v, vs.at[4], vr.at[4], top_peer)

    def stage_a(n, pieces):
        @pl.when(own_column(n))
        def _():
            j = block_of(n)
            for k in pieces:
                z_copy(j, k).wait_recv()
                x_copy(j, k).start()
                c_copy(n, k).start()

                @pl.when(goes_on(n))
                def _():
                    z_copy(j, k).start()

    def stage_b(n):
        j = block_of(n)
        for k in range(parts):
            x_copy(j, k).wait_recv()
            c_copy(n, k).start()

    def sends_done(n):
        j = block_of(n)

        @pl.when(jnp.logical_or(own_column(n), by_x(n)))
        def _():
            for k in range(parts):
                c_copy(n, k).wait_send()

        @pl.when(own_column(n))
        def _():
            for k in range(parts):
                x_copy(j, k).wait_send()

            @pl.when(goes_on(n))
            def _():
                for k in range(parts):
                    z_copy(j, k).wait_send()

    def r1_copy(n):
        j = key_of(n)
        return remote(
            lat_rows(part_of(n), peer_half, half), crx.at[j], r1s.at[j], r1r.at[j], core_peer
        )

    def rows_of(yy, k):
        return pl.ds(pl.multiple_of(c * half + yy * piece + k * sub, sub), sub)

    def chunk(k):
        return pl.ds(k * sub, sub)

    def y_copy(n, d, k):
        j = key_of(n)
        yy = (y + d) % ny
        return remote(
            lat_all.at[part_of(n), rows_of(yy, k)], yrx.at[j, d - 1, chunk(k)],
            ys.at[n % 4, d - 1, k], yr.at[n % 4, d - 1, k], {"sp": i, "tp": yy * 2 + c},
        )

    def xr_copy(n, k):
        j = block_of(n)
        return remote(
            lat_all.at[part_of(n), rows_of(y, k)], xrx.at[j, chunk(k)], xrs.at[j // 2, k],
            xrr.at[j // 2, k], x_peer,
        )

    def o_copy(n, k):
        return remote(
            lat_all.at[part_of(n), rows_of(y, k)], orx.at[z, chunk(k)], ors.at[block_of(n) // 2, k],
            orr.at[z, k],
            {"sp": block_of(n), "tp": t},
        )

    def v_copy(n, k):
        return remote(
            lat_all.at[part_of(n), rows_of(y, k)], orx.at[nz, chunk(k)], ors.at[1, k],
            orr.at[nz, k], x_peer,
        )

    def o_wait(zz, k):
        return remote(
            lat_all.at[i, rows_of(y, k)], orx.at[zz, chunk(k)], ors.at[0, k], orr.at[zz, k], x_peer
        )

    def stage_r2(n):
        j = key_of(n)
        b = part_of(n)
        r1_copy(n).wait_recv()

        def add_core(yy, k):
            at = pl.ds(pl.multiple_of(yy * piece + k * sub, sub), sub)
            lat_all[b, rows_of(yy, k), :] = lat_all[b, rows_of(yy, k), :] + crx[j, at, :]

        for k in range(chunks):
            for d in range(1, ny):
                add_core((y + d) % ny, k)
                y_copy(n, d, k).start()
        for k in range(chunks):
            add_core(y, k)

    def stage_r3(n):
        j = key_of(n)
        b = part_of(n)
        for k in range(chunks):
            total = lat_all[b, rows_of(y, k), :].astype(F32)
            for d in range(1, ny):
                y_copy(n, d, k).wait_recv()
                total = total + yrx[j, d - 1, k * sub : (k + 1) * sub, :].astype(F32)

            @pl.when(n == 0)
            def _():
                own_acc[k * sub : (k + 1) * sub, :] = total

            @pl.when(jnp.logical_and(is_low, n == base + 1))
            def _():
                own_acc[k * sub : (k + 1) * sub, :] += total

            @pl.when(n > 0)
            def _():
                lat_all[b, rows_of(y, k), :] = total.astype(BF16)

            @pl.when(for_x_sum(n))
            def _():
                xr_copy(n, k).start()

            @pl.when(in_plane(n))
            def _():
                o_copy(n, k).start()

            @pl.when(visit_out(n))
            def _():
                v_copy(n, k).start()

        for k in range(chunks):
            for d in range(1, ny):
                y_copy(n, d, k).wait_send()
        r1_copy(n).wait_send()

    def stage_r4(n):
        @pl.when(own_column(n))
        def _():
            j = block_of(n)
            b = part_of(n)
            for k in range(chunks):
                xr_copy(n, k).wait_recv()
                total = (
                    lat_all[b, rows_of(y, k), :].astype(F32)
                    + xrx[j, k * sub : (k + 1) * sub, :].astype(F32)
                )
                lat_all[b, rows_of(y, k), :] = total.astype(BF16)
                o_copy(n, k).start()

    def prepare(qi, q_ref):
        for h in range(heads):
            qh = jnp.concatenate(
                [q_ref[:, h * width : (h + 1) * width], jnp.zeros((rows, WIDE - width), BF16)], axis=1
            )
            qs_s[qi, h] = qh
            qt_s[qi, h] = qh.T
            gt_s[qi, h] = g_v[qi, :, h * VDIM : (h + 1) * VDIM].T
        dqt_s[qi] = jnp.zeros_like(dqt_s[qi])

    for cp in loads[:2]:
        cp.wait()

    @pl.when(is_top)
    def _():
        for k in range(3):
            visit_copy(k).start()

    for cp in loads[2:]:
        cp.wait()
    prepare(0, q_v)
    for h in range(heads):
        at = ao_v[:, h * VDIM : (h + 1) * VDIM].T
        delta_s[0, h : h + 1, :] = jnp.sum(
            gt_s[0, h].astype(F32) * at.astype(F32), axis=0, keepdims=True
        )
    lse_s[0] = lse_ref[...]

    @pl.when(is_top)
    def _():
        visit_copy(3).start()

    dvw_acc[...] = jnp.zeros_like(dvw_acc)

    def slot(n, diagonal):
        j = block_of(n)
        b = part_of(n)
        qi = lax.select(visiting(n), jnp.int32(1), jnp.int32(0))

        if not diagonal:

            @pl.when(jnp.logical_or(own_column(n), by_x(n)))
            def _():
                for k in range(parts):
                    c_copy(n, k).wait_recv()

            @pl.when(n == base + 1)
            def _():
                for k in range(4):
                    visit_copy(k).wait_recv()
                prepare(1, fq_v)

        rope = lat_all[j, :, latent_dim:]
        rope_t = rope.T[:ROPE]
        lat_t[...] = lat_all[j, :, :latent_dim].T
        keys = dot_nn(lat_all[j, :, :latent_dim], wk_v[...]).astype(BF16)
        v_s[...] = dot_nn(lat_all[j, :, :latent_dim], wv_v[...]).astype(BF16)
        for h in range(heads):
            kc = jnp.concatenate([keys[:, h * NOPE : (h + 1) * NOPE], rope], axis=1)
            kc_s[h] = kc
            kct_s[h, :NOPE] = keys[:, h * NOPE : (h + 1) * NOPE].T
            kct_s[h, NOPE:] = rope_t
        rope_sum = jnp.zeros((rows, WIDE - NOPE), F32)
        for h in range(heads):
            s = dot_nn(kc_s[h], qt_s[qi, h])
            zz = s * (scale * LOG2E) - lse_s[qi, h : h + 1, :] * LOG2E
            if diagonal:
                k_pos = lax.broadcasted_iota(jnp.int32, (rows, rows), 0)
                q_pos = lax.broadcasted_iota(jnp.int32, (rows, rows), 1)
                zz = jnp.where(k_pos <= q_pos, zz, -1e30)
            p = jnp.exp2(zz)
            dp = dot_nn(v_s[:, h * VDIM : (h + 1) * VDIM], gt_s[qi, h])
            ds = (p * (dp - delta_s[qi, h : h + 1, :])).astype(BF16)
            dv_s[:, h * VDIM : (h + 1) * VDIM] = dot_nn(
                p.astype(BF16), g_v[qi, :, h * VDIM : (h + 1) * VDIM]
            ).astype(BF16)
            dk = scale * dot_nn(ds, qs_s[qi, h])
            dk_s[:, h * NOPE : (h + 1) * NOPE] = dk[:, :NOPE].astype(BF16)
            rope_sum = rope_sum + dk[:, NOPE:]
            dqt_s[qi, h] += dot_nn(kct_s[h], ds)
            if h == heads // 2 - 1 and not diagonal:
                stage_r2(n - 1)

                @pl.when(n > 1)
                def _():
                    stage_a(n + 1, late)

        if not diagonal:

            @pl.when(n > 1)
            def _():
                stage_r3(n - 2)
                sends_done(n - 1)

                @pl.when(n > 4)
                def _():
                    stage_r4(n - 4)

                @pl.when(in_plane(n + 1))
                def _():
                    stage_b(n + 1)

        dlat = dot_nt(dk_s[...], wk_v[...]) + dot_nt(dv_s[...], wv_v[...])
        lat_all[b, :, :latent_dim] = dlat.astype(BF16)
        lat_all[b, :, latent_dim:] = rope_sum.astype(BF16)
        r1_copy(n).start()

        if diagonal:
            stage_a(n + 1, range(parts))

        @pl.when(jnp.logical_and(by_x(n + 1), jnp.logical_or(is_low, jnp.logical_not(in_plane(n + 1)))))
        def _():
            stage_b(n + 1)

        dvw_acc[...] += dot_nn(lat_t[...], dv_s[...])

        if not diagonal:
            stage_a(n + 2, early)

            @pl.when(jnp.logical_and(jnp.logical_and(x == 0, z > 0), n == 2))
            def _():
                for k in late:
                    x_copy(i, k).start()

    slot(jnp.int32(0), True)

    def later_slot(n, carry):
        slot(n, False)
        return carry

    lax.fori_loop(1, last + 1, later_slot, 0)

    @pl.when(is_low)
    def _():
        for h in range(heads):
            fq_v[:, h * width : (h + 1) * width] = (scale * dqt_s[1, h]).T.astype(BF16)
        back_copy().start()

    def wrows(k):
        return pl.ds(pl.multiple_of(k * lrows, lrows), lrows)

    def dvx_copy(d):
        zz = (z + d) % nz
        return remote(dvw_b.at[1 - x, zz], dvx_rx.at[zz], dvxs.at[d], dvxr.at[d], x_peer)

    send_order = tuple(range(1, nz)) + (0,)

    def dv_copy(d):
        zz = (z + d) % nz
        return remote(
            dvw_b.at[x, zz], dvw_rx.at[nz - d], dvs.at[d], dvr.at[nz - d], {"sp": 2 * zz + x, "tp": t}
        )

    def dv_wait(d):
        return remote(dvw_b.at[x, z], dvw_rx.at[d], dvs.at[d], dvr.at[d], x_peer)

    for k in range(ns):
        dvw_b[k % 2, k // 2] = dvw_acc[k * lrows : (k + 1) * lrows, :].astype(BF16)

    stage_r2(last)

    @pl.when(last > 3)
    def _():
        stage_r4(last - 3)

    @pl.when(last > 0)
    def _():
        stage_r3(last - 1)

    @pl.when(x == 1)
    def _():
        for d in send_order:
            dvx_copy(d).start()

    @pl.when(jnp.logical_and(x == 1, last > 2))
    def _():
        stage_r4(last - 2)

    @pl.when(jnp.logical_not(is_top))
    def _():
        for h in range(heads):
            q_v[:, h * width : (h + 1) * width] = (
                (scale * dqt_s[0, h]).T.astype(BF16)
            )

    stage_r3(last)

    @pl.when(x == 0)
    def _():
        for d in send_order:
            dvx_copy(d).start()

    def tail(n, carry):
        stage_r4(n)
        return carry

    lax.fori_loop(lax.max(last - 2 + x, 1), lower + 1, tail, 0)
    for d in range(1, nz):
        dvx_copy(d).wait_recv()
        zz = (z + d) % nz
        dvw_b[x, zz] = (dvw_acc[wrows(2 * zz + x), :] + dvx_rx[zz].astype(F32)).astype(BF16)
        dv_copy(d).start()

    @pl.when(is_top)
    def _():
        for k in range(4):
            visit_copy(k).wait_send()
        back_copy().wait_recv()
        for h in range(heads):
            q_v[:, h * width : (h + 1) * width] = (
                (scale * dqt_s[0, h]).T
                + fq_v[:, h * width : (h + 1) * width].astype(F32)
            ).astype(BF16)

    dq_out = pltpu.make_async_copy(q_v, dq_hbm, ld.at[2])
    dq_out.start()

    def ag_y(d, k):
        yy = (y + d) % ny
        return remote(
            fin.at[rows_of(y, k)], fin.at[rows_of(y, k)], ags.at[d - 1, k], agr.at[d - 1, k],
            {"sp": i, "tp": yy * 2 + c},
        )

    def ag_y_wait(d, k):
        yy = (y + ny - d) % ny
        return remote(
            fin.at[rows_of(yy, k)], fin.at[rows_of(yy, k)], ags.at[d - 1, k], agr.at[d - 1, k],
            {"sp": i, "tp": yy * 2 + c},
        )

    for k in range(chunks):

        def add(zz, carry):
            o_wait(zz, k).wait_recv()
            own_acc[k * sub : (k + 1) * sub, :] += orx[zz, k * sub : (k + 1) * sub, :].astype(F32)
            return carry

        @pl.when(x == 0)
        def _():
            add(z, 0)

        @pl.when(is_low)
        def _():
            add(nz, 0)

        lax.fori_loop(z + 1, lax.select(is_low, jnp.int32(top), jnp.int32(nz)), add, 0)
        fin[rows_of(y, k), :] = own_acc[k * sub : (k + 1) * sub, :].astype(BF16)
        for d in range(1, ny):
            ag_y(d, k).start()

    def ag_c(d):
        at = pl.ds(pl.multiple_of(c * half + (y + ny - d) % ny * piece, piece), piece)
        return remote(fin.at[at], fin.at[at], acs.at[d], acr.at[d], core_peer)

    def ag_c_wait(d):
        at = pl.ds(pl.multiple_of((1 - c) * half + (y + ny - d) % ny * piece, piece), piece)
        return remote(fin.at[at], fin.at[at], acs.at[d], acr.at[d], core_peer)

    ag_c(0).start()
    for d in range(1, ny):
        for k in range(chunks):
            ag_y_wait(d, k).wait_recv()
        ag_c(d).start()

    def out_copy(at, k):
        return pltpu.make_async_copy(
            fin.at[pl.ds(at, half), pl.ds(0, latent_dim)], dlat_hbm.at[pl.ds(at, half)], ld.at[k]
        )

    out_copy(my_half, 0).start()
    dvx_copy(0).wait_recv()
    dvw = dvw_acc[wrows(i), :] + dvx_rx[z].astype(F32)
    for d in range(1, nz):
        dv_wait(d).wait_recv()
        dvw = dvw + dvw_rx[d].astype(F32)
    dvw_o[...] = dvw
    dvw_out = pltpu.make_async_copy(dvw_o, dvw_hbm, ld.at[3])
    dvw_out.start()

    @pl.when(last > 0)
    def _():
        sends_done(last)

    @pl.when(has_next)
    def _():
        for k in range(parts):
            z_copy(i, k).wait_send()

    @pl.when(jnp.logical_or(x == 0, is_low))
    def _():
        for k in range(parts):
            x_copy(i, k).wait_send()

    @pl.when(is_low)
    def _():
        back_copy().wait_send()

    def drain(n, carry):
        @pl.when(jnp.logical_or(own_column(n), in_plane(n)))
        def _():
            for k in range(chunks):
                o_copy(n, k).wait_send()

        @pl.when(for_x_sum(n))
        def _():
            for k in range(chunks):
                xr_copy(n, k).wait_send()

        @pl.when(visit_out(n))
        def _():
            for k in range(chunks):
                v_copy(n, k).wait_send()

        return carry

    lax.fori_loop(1, last + 1, drain, 0)
    for d in range(1, nz):
        dv_copy(d).wait_send()
    for d in range(nz):
        dvx_copy(d).wait_send()
    for k in range(chunks):
        for d in range(1, ny):
            ag_y(d, k).wait_send()
    for d in range(ny):
        ag_c_wait(d).wait_recv()
    out_copy(peer_half, 1).start()
    drope_o[...] = fin[:, latent_dim : latent_dim + ROPE].astype(F32).T
    drope_out = pltpu.make_async_copy(drope_o, drope_hbm, ld.at[4])
    drope_out.start()
    for d in range(ny):
        ag_c(d).wait_send()
    with jax.named_scope("outs"):
        dq_out.wait()
        dvw_out.wait()
        out_copy(my_half, 0).wait()
        out_copy(peer_half, 1).wait()
        drope_out.wait()


def fused_backward(ns, tp, queries, out_grad, attn_out, lse, latent, rope_t, key_weight, value_weight):
    rows = queries.shape[0]
    latent_dim, hv = key_weight.shape
    heads = hv // NOPE
    packed = latent_dim + WIDE - NOPE
    lrows = latent_dim // ns
    ny = tp // 2
    chunks = min(4, rows // tp // 32)
    parts = chunks
    hbm = pl.BlockSpec(memory_space=pl.ANY)
    vmem = pl.BlockSpec(memory_space=pltpu.VMEM)
    dma = pltpu.SemaphoreType.DMA
    return pl.pallas_call(
        functools.partial(fused_kernel, ns, tp, heads, latent_dim),
        in_specs=[hbm, hbm, hbm, vmem, hbm, vmem, hbm, hbm],
        out_specs=[hbm, hbm, hbm, hbm],
        out_shape=[
            jax.ShapeDtypeStruct(queries.shape, BF16),
            jax.ShapeDtypeStruct(latent.shape, BF16),
            jax.ShapeDtypeStruct(rope_t.shape, F32),
            jax.ShapeDtypeStruct((lrows, hv), F32),
        ],
        scratch_shapes=[
            pltpu.VMEM(queries.shape, BF16),
            pltpu.VMEM((2,) + out_grad.shape, BF16),
            pltpu.VMEM(queries.shape, BF16),
            pltpu.VMEM((2, heads, rows), F32),
            pltpu.VMEM(attn_out.shape, BF16),
            pltpu.VMEM(key_weight.shape, BF16),
            pltpu.VMEM(value_weight.shape, BF16),
            pltpu.VMEM((2, heads, rows, WIDE), BF16),
            pltpu.VMEM((2, heads, WIDE, rows), BF16),
            pltpu.VMEM((2, heads, VDIM, rows), BF16),
            pltpu.VMEM((2, heads, NOPE + ROPE, rows), F32),
            pltpu.VMEM((2, heads, rows), F32),
            pltpu.VMEM((heads, rows, WIDE), BF16),
            pltpu.VMEM((heads, NOPE + ROPE, rows), BF16),
            pltpu.VMEM((latent_dim, rows), BF16),
            pltpu.VMEM((rows, hv), BF16),
            pltpu.VMEM((rows, hv), BF16),
            pltpu.VMEM((rows, hv), BF16),
            pltpu.VMEM((latent_dim, hv), F32),
            pltpu.VMEM((2, ns // 2, lrows, hv), BF16),
            pltpu.VMEM((ns // 2, lrows, hv), BF16),
            pltpu.VMEM((ns // 2, lrows, hv), BF16),
            pltpu.VMEM((ns + 2, rows, packed), BF16),
            pltpu.VMEM((ns, rows // 2, packed), BF16),
            pltpu.VMEM((ns, max(ny - 1, 1), rows // tp, packed), BF16),
            pltpu.VMEM((ns, rows // tp, packed), BF16),
            pltpu.VMEM((ns // 2 + 1, rows // tp, packed), BF16),
            pltpu.VMEM((rows // tp, packed), F32),
            pltpu.VMEM((rows, packed), BF16),
            pltpu.VMEM((lrows, hv), F32),
            pltpu.VMEM(rope_t.shape, F32),
            dma((6,)),
            dma((ns // 2, parts)),
            dma((3, parts)),
            dma((ns // 2, parts)),
            dma((3, parts)),
            dma((4, parts)),
            dma((4, parts)),
            dma((ns // 2, chunks)),
            dma((ns // 2, chunks)),
            dma((ns,)),
            dma((ns,)),
            dma((4, max(ny - 1, 1), chunks)),
            dma((4, max(ny - 1, 1), chunks)),
            dma((ns // 2 + 1, chunks)),
            dma((ns // 2, chunks)),
            dma((ns // 2,)),
            dma((ns // 2,)),
            dma((ns // 2,)),
            dma((ns // 2,)),
            dma((max(ny - 1, 1), chunks)),
            dma((max(ny - 1, 1), chunks)),
            dma((ny,)),
            dma((ny,)),
            dma((5,)),
            dma((5,)),
        ],
        compiler_params=pltpu.CompilerParams(
            collective_id=0, has_side_effects=True, vmem_limit_bytes=67043328
        ),
    )(queries, out_grad, attn_out, lse, latent, rope_t, key_weight, value_weight)


def finish_kernel(dq_ref, dlat_ref, drope_ref, dvw_ref, dq_out, dlat_out, drope_out, dvw_out):
    dq_out[...] = dq_ref[...]
    dlat_out[...] = dlat_ref[...].astype(F32)
    drope_out[...] = drope_ref[...]
    dvw_out[...] = dvw_ref[...]


def finish(dq, dlat, drope_t, dvw):
    steps = 2

    def rows_of(a):
        return pl.BlockSpec((a.shape[0] // steps, a.shape[1]), lambda k: (k, 0))

    specs = [rows_of(a) for a in (dq, dlat, drope_t, dvw)]
    return pl.pallas_call(
        finish_kernel,
        grid=(steps,),
        in_specs=specs,
        out_specs=specs,
        out_shape=[
            jax.ShapeDtypeStruct(dq.shape, BF16),
            jax.ShapeDtypeStruct(dlat.shape, F32),
            jax.ShapeDtypeStruct(drope_t.shape, F32),
            jax.ShapeDtypeStruct(dvw.shape, F32),
        ],
        compiler_params=pltpu.CompilerParams(dimension_semantics=("arbitrary",)),
    )(dq, dlat, drope_t, dvw)


def per_device(queries, latent, rope_key, key_weight, value_weight, log_sums, attn_out, out_grad):
    d_queries, dlat, drope_t, d_value_weight = fused_backward(
        lax.axis_size("sp"), lax.axis_size("tp"),
        queries, out_grad, attn_out, log_sums, latent, rope_key.T, key_weight, value_weight,
    )
    d_queries, d_latent, drope_t, d_value_weight = finish(d_queries, dlat, drope_t, d_value_weight)
    d_rope = drope_t.T
    return (d_queries, d_latent, d_rope, d_value_weight)


def solution(mesh):
    placed = (
        P("sp", "tp"),
        P("sp", None),
        P("sp", None),
        P(None, "tp"),
        P(None, "tp"),
        P("tp", "sp"),
        P("sp", "tp"),
        P("sp", "tp"),
    )
    return jax.shard_map(
        per_device,
        mesh=mesh,
        in_specs=placed,
        out_specs=(P("sp", "tp"), P("sp", None), P("sp", None), P("sp", "tp")),
        check_vma=False,
    )
```
